256 devices in a mesh: sp: 32 (over z, x), tp: 8 (over y, core).
Axes of the slice: x: 4, y: 4, z: 8, core: 2. Of those that a mesh axis runs over, the one named last changes fastest.
Arguments:
- tokens: bfloat16 [12288, 2048], P(('sp', 'tp')), may hold values from -6 to 6
- norm_gain: bfloat16 [2048], replicated, may hold values from 0.099609375 to 1.8984375
- query_down_weight: bfloat16 [2048, 512], replicated, may hold values from -0.125 to 0.125
- query_latent_norm_gain: bfloat16 [512], replicated, may hold values from 0.099609375 to 1.8984375
- key_value_down_weight: bfloat16 [2048, 256], replicated, may hold values from -0.125 to 0.125
- key_value_latent_gain: bfloat16 [256], replicated, may hold values from 0.099609375 to 1.8984375
- w_rope_key: bfloat16 [2048, 32], replicated, may hold values from -0.125 to 0.125
- w_pool_in: bfloat16 [2048, 512], replicated, may hold values from -0.125 to 0.125
- query_up_weight: bfloat16 [512, 2304], P(None, 'tp'), may hold values from -0.25 to 0.25
- key_value_up_weight: bfloat16 [256, 3072], P(None, 'tp'), may hold values from -0.375 to 0.375
- query_gain: bfloat16 [96], replicated, may hold values from 1 to 16
- key_gain: bfloat16 [96], replicated, may hold values from 1 to 16
- w_pool_mix: bfloat16 [8, 64, 64], P('tp'), may hold values from -0.75 to 0.75
- pool_scale: bfloat16 [512], P('tp'), may hold values from 1 to 10
- w_out_attn: bfloat16 [1536, 2048], P('tp'), may hold values from -0.3125 to 0.3125
- w_out_pool: bfloat16 [512, 2048], P('tp'), may hold values from -0.25 to 0.25
Outputs:
- mixed: bfloat16 [12288, 2048], P(('sp', 'tp'))
- row_logsum: float32 [24, 12288], P('tp', 'sp')
The draws below stay inside these ranges and needn't reach their ends.
All inputs are finite; a program needn't handle non-finite values.
Results may differ from the reference program's by a relative error of at most 0.035.
Values may be sent and summed in bfloat16 or wider, within the bound.
A program may use at most 128 MiB of HBM per device.

```python
import math
import jax
import jax.numpy as jnp
from jax import lax

MODEL_WIDTH = 2048
HEAD_COUNT = 24
PLAIN_HEAD_SIZE = 64
ROTARY_SIZE = 32
VALUE_HEAD_SIZE = 64
QUERY_RANK = 512
KEY_VALUE_RANK = 256
GROUPS = 8
GDIM = 64
TOKENS = 12288
N_TP = 8


def head_gain(key, salt):
    base = jax.random.uniform(jax.random.fold_in(key, salt), (PLAIN_HEAD_SIZE + ROTARY_SIZE,), jnp.float32, 1.0, 2.0)
    return base.astype(jnp.bfloat16)


def draw_query_gain(key, part):
    return head_gain(key, 1)


def draw_key_gain(key, part):
    return head_gain(key, 2)


def levels(rng, shape, split, least, high):
    level, own = 1.0, jax.random.fold_in(rng, 6)
    for dim, parts in split:
        draws = jnp.exp(jax.random.uniform(jax.random.fold_in(own, dim), (parts,), jnp.float32, least / len(split), high / len(split)))
        level = level * jnp.repeat(draws, shape[dim] // parts).reshape([-1 if axis == dim else 1 for axis in range(len(shape))])
    return level


def noise(rng, shape, spread, limit, split=(), held_as=jnp.bfloat16):
    level = levels(rng, shape, split, -0.22, 0.18) if split else 1.0
    values = jax.random.normal(rng, shape, jnp.float32) * spread * level
    return jnp.minimum(jnp.maximum(values, -limit), limit).astype(held_as)


def setup_inputs(seed: int = 0) -> dict:
    arg_keys = jax.random.split(jax.random.key(seed), 17)
    return {
        "tokens": noise(arg_keys[0], (TOKENS, MODEL_WIDTH), 1.0, 6.0, ((0, 256),)),
        "norm_gain": jnp.clip(1.0 + 0.18 * jax.random.normal(arg_keys[1], (MODEL_WIDTH,), jnp.float32), 0.099609375, 1.8984375).astype(jnp.bfloat16),
        "query_down_weight": noise(arg_keys[2], (MODEL_WIDTH, QUERY_RANK), MODEL_WIDTH ** -0.5, 0.125),
        "query_latent_norm_gain": jnp.clip(1.0 + 0.18 * jax.random.normal(arg_keys[3], (QUERY_RANK,), jnp.float32), 0.099609375, 1.8984375).astype(jnp.bfloat16),
        "key_value_down_weight": noise(arg_keys[4], (MODEL_WIDTH, KEY_VALUE_RANK), MODEL_WIDTH ** -0.5, 0.125),
        "key_value_latent_gain": jnp.clip(1.0 + 0.18 * jax.random.normal(arg_keys[5], (KEY_VALUE_RANK,), jnp.float32), 0.099609375, 1.8984375).astype(jnp.bfloat16),
        "w_rope_key": noise(arg_keys[6], (MODEL_WIDTH, ROTARY_SIZE), MODEL_WIDTH ** -0.5, 0.125),
        "w_pool_in": noise(arg_keys[7], (MODEL_WIDTH, GROUPS * GDIM), MODEL_WIDTH ** -0.5, 0.125),
        "query_up_weight": noise(arg_keys[8], (QUERY_RANK, HEAD_COUNT * (PLAIN_HEAD_SIZE + ROTARY_SIZE)), QUERY_RANK ** -0.5, 0.25, ((1, 8),)),
        "key_value_up_weight": noise(arg_keys[9], (KEY_VALUE_RANK, HEAD_COUNT * (PLAIN_HEAD_SIZE + VALUE_HEAD_SIZE)), KEY_VALUE_RANK ** -0.5, 0.375, ((1, 8),)),
        "query_gain": draw_query_gain(jax.random.fold_in(arg_keys[16], 71), 0),
        "key_gain": draw_key_gain(jax.random.fold_in(arg_keys[16], 71), 0),
        "w_pool_mix": noise(arg_keys[12], (GROUPS, GDIM, GDIM), GDIM ** -0.5, 0.75, ((0, 8),)),
        "pool_scale": jnp.clip(jnp.exp(math.log(10.0) - 2.3025851 * jax.random.uniform(arg_keys[13], (GROUPS * GDIM,), jnp.float32) ** levels(arg_keys[13], (GROUPS * GDIM,), ((0, 8),), -0.2, 0.2)), 1.0, 10.0).astype(jnp.bfloat16),
        "w_out_attn": noise(arg_keys[14], (HEAD_COUNT * VALUE_HEAD_SIZE, MODEL_WIDTH), (HEAD_COUNT * VALUE_HEAD_SIZE // 4) ** -0.5, 0.3125, ((0, 8),)),
        "w_out_pool": noise(arg_keys[15], (GROUPS * GDIM, MODEL_WIDTH), (GROUPS * GDIM) ** -0.5, 0.25, ((0, 8),)),
    }


epsilon = 1e-06
rope_base = 10000.0
query_rows = 128

def norm_rows(values, gain):
    mean_square = lax.optimization_barrier(jnp.mean(values * values, axis=-1, keepdims=True))
    return values * lax.rsqrt(mean_square + epsilon) * gain.astype(jnp.float32)

def rotate_tail(values, positions):
    half = ROTARY_SIZE // 2
    freqs = rope_base ** (-jnp.arange(half, dtype=jnp.float32) / half)
    angles = positions[:, None] * freqs[None, :]
    cosine = jnp.cos(angles)[:, None, :]
    sine = jnp.sin(angles)[:, None, :]
    first = values[..., PLAIN_HEAD_SIZE:PLAIN_HEAD_SIZE + half]
    second = values[..., PLAIN_HEAD_SIZE + half:]
    return jnp.concatenate([values[..., :PLAIN_HEAD_SIZE], first * cosine - second * sine, first * sine + second * cosine], axis=-1)

def reference(tokens, norm_gain, query_down_weight, query_latent_norm_gain, key_value_down_weight, key_value_latent_gain, w_rope_key, w_pool_in, query_up_weight, key_value_up_weight, query_gain, key_gain, w_pool_mix, pool_scale, w_out_attn, w_out_pool):
    length = tokens.shape[0]
    normed = norm_rows(tokens.astype(jnp.float32), norm_gain).astype(jnp.bfloat16)
    query_latent = norm_rows(jnp.dot(normed, query_down_weight, preferred_element_type=jnp.float32), query_latent_norm_gain).astype(jnp.bfloat16)
    kv_latent = norm_rows(jnp.dot(normed, key_value_down_weight, preferred_element_type=jnp.float32), key_value_latent_gain).astype(jnp.bfloat16)
    rope_key = jnp.dot(normed, w_rope_key, preferred_element_type=jnp.float32).astype(jnp.bfloat16)
    pool_input = jnp.dot(normed, w_pool_in, preferred_element_type=jnp.float32).astype(jnp.bfloat16)
    positions = jnp.arange(length, dtype=jnp.int32).astype(jnp.float32)
    query_vectors = jnp.dot(query_latent, query_up_weight, preferred_element_type=jnp.float32).reshape(length, HEAD_COUNT, PLAIN_HEAD_SIZE + ROTARY_SIZE)
    query_vectors = rotate_tail(norm_rows(query_vectors, query_gain), positions).astype(jnp.bfloat16)
    key_value_pair = jnp.dot(kv_latent, key_value_up_weight, preferred_element_type=jnp.float32).reshape(length, HEAD_COUNT, PLAIN_HEAD_SIZE + VALUE_HEAD_SIZE)
    shared = jnp.broadcast_to(rope_key.astype(jnp.float32)[:, None, :], (length, HEAD_COUNT, ROTARY_SIZE))
    keys = jnp.concatenate([key_value_pair[..., :PLAIN_HEAD_SIZE], shared], axis=-1)
    keys = rotate_tail(norm_rows(keys, key_gain), positions).astype(jnp.bfloat16)
    values = key_value_pair[..., PLAIN_HEAD_SIZE:].astype(jnp.bfloat16)
    scale = (PLAIN_HEAD_SIZE + ROTARY_SIZE) ** (-0.5)
    key_float = keys.astype(jnp.float32)
    value_float = values.astype(jnp.float32)
    query_blocks = query_vectors.astype(jnp.float32).reshape(length // query_rows, query_rows, HEAD_COUNT, PLAIN_HEAD_SIZE + ROTARY_SIZE)

    def attend(query_block):
        scores = jnp.einsum('qhd,khd->hqk', query_block, key_float) * scale
        row_max = lax.optimization_barrier(jnp.max(scores, axis=-1))
        exp_scores = jnp.exp(scores - row_max[:, :, None])
        row_total = lax.optimization_barrier(jnp.sum(exp_scores, axis=-1))
        weights = lax.optimization_barrier(exp_scores.astype(jnp.bfloat16)).astype(jnp.float32)
        summed = jnp.einsum('hqk,khd->qhd', weights, value_float)
        output = (summed / jnp.transpose(row_total)[:, :, None]).astype(jnp.bfloat16)
        return (output, row_max + jnp.log(row_total))
    outputs, logsums = lax.map(attend, query_blocks)
    attention = outputs.reshape(length, HEAD_COUNT * VALUE_HEAD_SIZE)
    row_logsum = jnp.transpose(logsums, (1, 0, 2)).reshape(HEAD_COUNT, length)
    pool_float = pool_input.astype(jnp.float32)
    running = jnp.concatenate([jnp.zeros((1, GROUPS * GDIM), jnp.float32), jnp.cumsum(pool_float, axis=0)], axis=0)
    places = jnp.arange(length, dtype=jnp.int32)
    pieces = []
    for group in range(GROUPS):
        half = 2 ** (group % 4)
        upper = jnp.minimum(places + half, length)
        lower = jnp.maximum(places - half, 0)
        first_col = group * GDIM
        window = running[upper, first_col:first_col + GDIM] - running[lower, first_col:first_col + GDIM]
        total_count = (upper - lower).astype(jnp.float32)[:, None]
        pooled = (window / total_count - pool_float[:, first_col:first_col + GDIM]).astype(jnp.bfloat16)
        mapped = jnp.dot(pooled, w_pool_mix[group], preferred_element_type=jnp.float32)
        pieces.append((mapped * pool_scale[first_col:first_col + GDIM].astype(jnp.float32)).astype(jnp.bfloat16))
    pool_out = jnp.concatenate(pieces, axis=1)
    head_cols = HEAD_COUNT * VALUE_HEAD_SIZE // N_TP
    pool_cols = GROUPS * GDIM // N_TP
    mixed = jnp.zeros((length, MODEL_WIDTH), jnp.float32)
    for member in range(N_TP):
        head_start = member * head_cols
        pool_start = member * pool_cols
        partial_sum = jnp.dot(attention[:, head_start:head_start + head_cols], w_out_attn[head_start:head_start + head_cols], preferred_element_type=jnp.float32)
        partial_sum = partial_sum + jnp.dot(pool_out[:, pool_start:pool_start + pool_cols], w_out_pool[pool_start:pool_start + pool_cols], preferred_element_type=jnp.float32)
        mixed = mixed + lax.optimization_barrier(partial_sum.astype(jnp.bfloat16)).astype(jnp.float32)
    return (mixed.astype(jnp.bfloat16), row_logsum)
```

```python
import numpy as np

import jax
import jax.numpy as jnp
from jax import lax
from jax.experimental import pallas as pl
from jax.experimental.pallas import tpu as pltpu
from jax.sharding import PartitionSpec as P

MESH = pl.DeviceIdType.MESH
BF, F32 = jnp.bfloat16, jnp.float32
H = 3
TB = 384
OWN = 48
NB = 32
LH = 160
PER = 4
STEPS = NB // PER
EPS = 1e-6
LOG2E = 1.4426950408889634
LN2 = 0.6931471805599453
LENGTH = NB * TB

ROW_ORDER = (0, -1, 1, -2, 2, -3, 3, 4)
X_TARGETS = ((0, 1), (0, -1), (0, 2))


def slot_of(dz, dx):
    dz = (dz + 3) % 8 - 3
    return 4 * ROW_ORDER.index(dz) + dx % 4


def forwards(core, dz, dx):
    if core == 0:
        if dz == 0:
            return (X_TARGETS if dx == 0 else ()) + ((1, 0), (-1, 0))
        if dz in (-1, -2) or (dz == -3 and dx in (0, 1)):
            return ((1, 0),)
        if dz in (1, 2) or (dz == 3 and dx in (2, 3)):
            return ((-1, 0),)
        return ()
    if dx:
        return ()
    if dz == 0:
        return ((1, 0), (-1, 0)) + X_TARGETS
    along = ((1, 0),) if dz in (-1, -2, -3) else ((-1, 0),) if dz in (1, 2) else ()
    return along + X_TARGETS


PLAN = tuple(
    {
        slot_of(dz, dx): tuple((az, ax, slot_of(dz - az, dx - ax)) for az, ax in forwards(core, dz, dx))
        for dz in ROW_ORDER
        for dx in range(4)
    }
    for core in (0, 1)
)
SERVICE = (
    tuple(tuple(range(4 * (p // 3), 4 * (p // 3) + 4)) if p % 3 == 0 else () for p in range(3 * STEPS)),
    tuple(tuple(range(4 * (p // 3), 4 * (p // 3) + 4)) if p % 3 == 0 else () for p in range(3 * STEPS)),
)


def dot(a, b, dims):
    return lax.dot_general(a, b, (dims, ((), ())), preferred_element_type=F32)


def remote(src, dst, send, recv, device):
    return pltpu.make_async_remote_copy(
        src_ref=src, dst_ref=dst, send_sem=send, recv_sem=recv, device_id=device, device_id_type=MESH
    )


def norm_rows(v, gain):
    return v * lax.rsqrt(jnp.mean(v * v, axis=-1, keepdims=True) + EPS) * gain


def column(row, count):
    n = row.shape[1]
    row = jnp.concatenate([row, jnp.zeros((1, 128 - n), F32)], axis=1)
    return jnp.tile(jnp.transpose(jnp.broadcast_to(row, (128, 128)))[:n], (1, count))


def prep(lat, w_ref, k_ref, v_ref, first):
    n = lat.shape[1]
    cols = slice(first, first + n)
    kv = dot(w_ref[...], lat[:256], ((1,), (0,)))
    rope = lat[256:288].astype(F32)
    rho = lat[288:304].astype(F32)
    rho = rho[0:1] + rho[1:2]
    for h in range(H):
        k = kv[h * 64 : (h + 1) * 64]
        r = lax.rsqrt((jnp.sum(k * k, axis=0, keepdims=True) + rho) * (1.0 / 96) + EPS)
        k_ref[h, 0:64, cols] = (k * r).astype(BF)
        k_ref[h, 64:96, cols] = (rope * r).astype(BF)
        v_ref[h, 0:64, cols] = kv[192 + h * 64 : 256 + h * 64].astype(BF)


def soften(h, s, m_ref, acc, v_ref):
    m_old = m_ref[h]
    m_new = jnp.maximum(m_old, jnp.broadcast_to(jnp.max(s, axis=1, keepdims=True), m_old.shape))
    m_ref[h] = m_new
    p = jnp.exp2(s - jnp.tile(m_new, (1, s.shape[1] // 128))).astype(BF)
    acc[h] = acc[h] * jnp.exp2(m_old - m_new) + dot(p, v_ref[h], ((1,), (1,)))


def layer(
    tok, h_wq, h_wkv, h_wr, h_wp, n_gain, q_gain, kv_gain, wq_up, wkv_up, hq_gain, hk_gain, tables,
    w_mix, p_scale, h_woa, h_wop,
    out, lse_out,
    w_q, w_kv, w_r, w_p, w_o, kvg, qg, psend, pool, halo, lat, qs, wup, k_ref, v_ref, m_ref, acc,
    pool_out, cat, pair_s, pair_r, own, row_s, row_r,
    w_sem, g_sem, lat_send, lat_recv, pair_recv, t_sem,
):
    sp, tp = lax.axis_index("sp"), lax.axis_index("tp")
    z, x = lax.div(sp, 4), lax.rem(sp, 4)
    y, c = lax.div(tp, 2), lax.rem(tp, 2)
    partner = tp + 1 - 2 * c

    def chip(az, ax):
        return lax.rem(z + az + 8, 8) * 4 + lax.rem(x + ax + 4, 4)

    weights = [
        pltpu.make_async_copy(a, b, w_sem.at[i])
        for i, (a, b) in enumerate(
            (
                (h_wkv, w_kv),
                (h_wr, w_r),
                (h_wq, w_q),
                (h_wp, w_p),
                (h_woa, w_o.at[pl.ds(0, 192)]),
                (h_wop, w_o.at[pl.ds(192, 64)]),
            )
        )
    ]
    for copy in weights:
        copy.start()

    barrier = pltpu.get_barrier_semaphore()
    friends = [(sp, lax.rem(tp + k, 8)) for k in range(1, 8)]
    friends += [(chip(az, ax), tp) for az, ax in X_TARGETS + ((1, 0), (-1, 0))]
    friends += [(lax.rem(sp + 1, NB), tp), (lax.rem(sp + NB - 1, NB), tp)]
    for friend in friends:
        pl.semaphore_signal(barrier, inc=1, device_id=friend, device_id_type=MESH)

    normed = norm_rows(tok[...].astype(F32), n_gain[...].astype(F32)).astype(BF)
    weights[0].wait()
    weights[1].wait()
    kv = norm_rows(dot(normed, w_kv[...], ((1,), (0,))), kv_gain[...].astype(F32))
    rope = dot(normed, w_r[...], ((1,), (0,)))
    kvg[tp] = jnp.concatenate([kv, rope, jnp.zeros((OWN, 96), F32)], axis=1).astype(BF)
    pl.semaphore_wait(barrier, len(friends))

    def spread(src, dst, kind):
        copies = []
        for k in (4, 3, 5, 2, 6, 1, 7):
            peer = lax.rem(tp + k, 8)
            copies.append(remote(src(peer), dst.at[tp], g_sem.at[kind, k], g_sem.at[kind + 1, 8 - k], (sp, peer)))
            copies[-1].start()
        return copies

    def gathered(dst, kind):
        for k in range(1, 8):
            peer = lax.rem(tp + k, 8)
            remote(dst.at[peer], dst.at[peer], g_sem.at[kind, k], g_sem.at[kind + 1, k], (sp, peer)).wait_recv()

    gathers = spread(lambda peer: kvg.at[tp], kvg, 0)
    weights[2].wait()
    qg[tp] = norm_rows(dot(normed, w_q[...], ((1,), (0,))), q_gain[...].astype(F32)).astype(BF)
    gathers += spread(lambda peer: qg.at[tp], qg, 2)
    weights[3].wait()
    pooled_in = dot(normed, w_p[...], ((1,), (0,))).astype(BF)
    for g in range(8):
        psend[g] = jnp.concatenate([pooled_in[:, g * 64 : (g + 1) * 64], jnp.zeros((OWN, 64), BF)], axis=1)
    pool[tp] = psend[tp]
    gathers += spread(lambda peer: psend.at[peer], pool, 4)

    up = jnp.transpose(wkv_up[...].astype(F32))
    for h in range(H):
        wup[h * 64 : (h + 1) * 64] = up[h * 128 : h * 128 + 64].astype(BF)
        wup[192 + h * 64 : 256 + h * 64] = up[h * 128 + 64 : h * 128 + 128].astype(BF)
    lanes = lax.broadcasted_iota(jnp.int32, (16, TB), 1)
    off_c = jnp.sum(jnp.where(lanes == sp, tables[2], 0.0), axis=1, keepdims=True)
    off_s = jnp.sum(jnp.where(lanes == sp, tables[3], 0.0), axis=1, keepdims=True)
    cosine = tables[0] * off_c - tables[1] * off_s
    sine = tables[1] * off_c + tables[0] * off_s
    kcol = column(hk_gain[...].astype(F32), 3)
    qcol = column(hq_gain[...].astype(F32), 3)
    m_ref[...] = jnp.full(m_ref.shape, -1e30, F32)
    acc[...] = jnp.zeros(acc.shape, F32)
    k_ref[...] = jnp.zeros(k_ref.shape, BF)
    v_ref[...] = jnp.zeros(v_ref.shape, BF)
    v_ref[:, 64:80, :] = jnp.ones((H, 16, v_ref.shape[2]), BF)

    gathered(kvg, 0)
    turned = jnp.transpose(kvg[...].reshape(TB, TB).astype(F32))
    rope = turned[256:288]
    rho = jnp.sum(rope * rope, axis=0, keepdims=True)
    rho_hi = rho.astype(BF).astype(F32)
    rope = rope * kcol[64:96]
    first, second = rope[:16], rope[16:]
    row = lax.broadcasted_iota(jnp.int32, (32, TB), 0)
    last = jnp.where(row == 0, rho_hi, jnp.where(row == 1, rho - rho_hi, 0.0))
    lat[0, 0] = turned[:LH].astype(BF)
    lat[0, 1] = jnp.concatenate(
        [turned[LH:256], first * cosine - second * sine, first * sine + second * cosine, last], axis=0
    ).astype(BF)

    def outgoing(core, s):
        copies = [
            remote(lat.at[s, core], lat.at[t, core], lat_send.at[s, k], lat_recv.at[t], (chip(az, ax), tp))
            for k, (az, ax, t) in enumerate(PLAN[core][s])
        ]
        if s:
            copies.append(
                remote(lat.at[s, core], lat.at[s, core], lat_send.at[s, 5], pair_recv.at[s], (sp, partner))
            )
        return copies

    def serve(point):
        for core in (0, 1):
            slots = SERVICE[core][point]
            if slots:

                @pl.when(c == core)
                def _():
                    for s in slots:
                        if s:
                            remote(
                                lat.at[s, core], lat.at[s, core], lat_send.at[s, 0], lat_recv.at[s], (sp, partner)
                            ).wait_recv()
                        for copy in outgoing(core, s):
                            copy.start()

    for core in (0, 1):

        @pl.when(c == core)
        def _():
            for copy in outgoing(core, 0):
                copy.start()

    gathered(pool, 4)
    halos = [
        remote(
            pool.at[7, pl.ds(32, 16)], halo.at[0], t_sem.at[0, 0], t_sem.at[1, 0], (lax.rem(sp + 1, NB), tp)
        ),
        remote(
            pool.at[0, pl.ds(0, 16)], halo.at[1], t_sem.at[0, 1], t_sem.at[1, 1], (lax.rem(sp + NB - 1, NB), tp)
        ),
    ]
    for copy in halos:
        copy.start()

    gathered(qg, 2)
    qt = dot(wq_up[...], qg[...].reshape(TB, 512), ((0,), (1,)))
    scale = 96.0 ** -0.5 * LOG2E
    for h in range(H):
        q = qt[h * 96 : (h + 1) * 96]
        q = q * (lax.rsqrt(jnp.mean(q * q, axis=0, keepdims=True) + EPS) * scale) * qcol
        first, second = q[64:80], q[80:96]
        q = jnp.concatenate(
            [
                q[:64] * kcol[:64],
                first * cosine - second * sine,
                first * sine + second * cosine,
                jnp.zeros((32, TB), F32),
            ],
            axis=0,
        )
        qs[h] = jnp.transpose(q).astype(BF)

    for copy in halos:
        copy.wait_recv()
    mine = pool[...].reshape(TB, 128)
    wide = jnp.concatenate([halo[0], mine, halo[1], jnp.zeros((96, 128), BF)], axis=0)
    half = jnp.left_shift(jnp.int32(1), lax.rem(tp, 4))
    here = lax.broadcasted_iota(jnp.int32, (TB, 512), 0)
    there = lax.broadcasted_iota(jnp.int32, (TB, 512), 1) - 16
    place = there + sp * TB
    band = (there >= here - half) & (there < here + half) & (place >= 0) & (place < LENGTH)
    summed = dot(jnp.where(band, 1.0, 0.0).astype(BF), wide, ((1,), (0,)))
    place = lax.broadcasted_iota(jnp.int32, (TB, 128), 0) + sp * TB
    count = jnp.minimum(place + half, LENGTH) - jnp.maximum(place - half, 0)
    pooled = (summed / count.astype(F32) - mine.astype(F32)).astype(BF)
    mapped = dot(pooled[:, :64], w_mix[0], ((1,), (0,)))
    pool_out[...] = (mapped * p_scale[...].astype(F32)).astype(BF)

    def step(i, carry):
        for k in range(STEPS):

            @pl.when(i == k)
            def _():
                if k:
                    serve(3 * k)
                else:
                    for core in (0, 1):

                        @pl.when(c == core)
                        def _():
                            for s in SERVICE[core][0]:
                                if s:
                                    remote(
                                        lat.at[s, core],
                                        lat.at[s, core],
                                        lat_send.at[s, 0],
                                        lat_recv.at[s],
                                        (sp, partner),
                                    ).wait_recv()
                                    for copy in outgoing(core, s):
                                        copy.start()

                for s in range(PER * k, PER * k + PER):
                    if s:
                        remote(
                            lat.at[s, 1 - c], lat.at[s, 1 - c], lat_send.at[s, 5], pair_recv.at[s], (sp, partner)
                        ).wait_recv()

        for j in range(PER):
            prep(lat[i * PER + j].reshape(2 * LH, TB), wup, k_ref, v_ref, j * TB)
        held = None
        for h in range(H):
            s = dot(qs[h], k_ref[h], ((1,), (0,)))
            if held is not None:
                soften(h - 1, held, m_ref, acc, v_ref)
            held = s
            if h < H - 1:
                for k in range(STEPS):
                    if any(SERVICE[core][3 * k + h + 1] for core in (0, 1)):

                        @pl.when(i == k)
                        def _():
                            serve(3 * k + h + 1)

        soften(H - 1, held, m_ref, acc, v_ref)
        return carry

    lax.fori_loop(0, STEPS, step, 0)

    lane = lax.broadcasted_iota(jnp.int32, (TB, 128), 1)
    parts, logs = [], jnp.zeros((TB, 128), F32)
    for h in range(H):
        o = acc[h]
        total = o[:, 64:65]
        parts.append((o[:, :64] / total).astype(BF))
        logs = jnp.where(lane == h, m_ref[h] * LN2 + jnp.log(total), logs)
    lse_out[...] = jnp.transpose(logs)[:H]
    cat[...] = jnp.concatenate(parts + [pool_out[...]], axis=1).reshape(8, OWN, 256)
    weights[4].wait()
    weights[5].wait()

    def rows_of(core):
        return jnp.concatenate([cat[2 * k + core] for k in range(4)], axis=0)

    pair_s[...] = dot(rows_of(1 - c), w_o[...], ((1,), (0,))).astype(BF).reshape(4, OWN, 2048)
    tails = []
    for k in (2, 1, 3, 0):
        there = lax.rem(y + k, 4)
        tails.append(
            remote(pair_s.at[there], pair_r.at[there], t_sem.at[2, k], t_sem.at[3, k], (sp, partner))
        )
        tails[-1].start()
    own[...] = dot(rows_of(c), w_o[...], ((1,), (0,))).reshape(4, OWN, 2048)
    sums = None
    for i, k in enumerate((2, 1, 3, 0)):
        there = lax.rem(y + k, 4)
        tails[i].wait_recv()
        value = own[there] + pair_r[there].astype(F32)
        if k:
            row_s[k - 1] = value.astype(BF)
            copy = remote(
                row_s.at[k - 1], row_r.at[3 - k], t_sem.at[4, k], t_sem.at[5, 4 - k], (sp, 2 * there + c)
            )
            copy.start()
            tails.append(copy)
        else:
            sums = value
    for k in (1, 3, 2):
        remote(row_s.at[k - 1], row_r.at[k - 1], t_sem.at[4, k], t_sem.at[5, k], (sp, partner)).wait_recv()
        sums = sums + row_r[k - 1].astype(F32)
    out[...] = sums.astype(BF)

    for copy in gathers + halos + tails:
        copy.wait_send()
    for core in (0, 1):

        @pl.when(c == core)
        def _():
            for s in range(NB):
                for copy in outgoing(core, s):
                    copy.wait_send()


def rotation_tables():
    half = 16
    freqs = 10000.0 ** (-np.arange(half, dtype=np.float64) / half)
    inside = freqs[:, None] * np.arange(TB)[None, :]
    blocks = np.zeros((half, TB))
    blocks[:, :NB] = freqs[:, None] * (TB * np.arange(NB))[None, :]
    return np.stack([np.cos(inside), np.sin(inside), np.cos(blocks), np.sin(blocks)]).astype(np.float32)


def shards(tokens, norm_gain, query_down_weight, query_latent_norm_gain, key_value_down_weight,
           key_value_latent_gain, w_rope_key, w_pool_in, query_up_weight, key_value_up_weight,
           query_gain, key_gain, w_pool_mix, pool_scale, w_out_attn, w_out_pool):
    vmem, anywhere = pl.BlockSpec(memory_space=pltpu.VMEM), pl.BlockSpec(memory_space=pl.ANY)
    dma, n = pltpu.SemaphoreType.DMA, PER * TB
    return pl.pallas_call(
        layer,
        out_shape=(jax.ShapeDtypeStruct((OWN, 2048), BF), jax.ShapeDtypeStruct((H, TB), F32)),
        in_specs=[vmem] + [anywhere] * 4 + [vmem] * 10 + [anywhere] * 2,
        out_specs=(vmem, vmem),
        scratch_shapes=[
            pltpu.VMEM((2048, 512), BF),
            pltpu.VMEM((2048, 256), BF),
            pltpu.VMEM((2048, 32), BF),
            pltpu.VMEM((2048, 512), BF),
            pltpu.VMEM((256, 2048), BF),
            pltpu.VMEM((8, OWN, TB), BF),
            pltpu.VMEM((8, OWN, 512), BF),
            pltpu.VMEM((8, OWN, 128), BF),
            pltpu.VMEM((8, OWN, 128), BF),
            pltpu.VMEM((2, 16, 128), BF),
            pltpu.VMEM((NB, 2, LH, TB), BF),
            pltpu.VMEM((H, TB, 128), BF),
            pltpu.VMEM((H * 128, 256), BF),
            pltpu.VMEM((H, 128, n), BF),
            pltpu.VMEM((H, 128, n), BF),
            pltpu.VMEM((H, TB, 128), F32),
            pltpu.VMEM((H, TB, 128), F32),
            pltpu.VMEM((TB, 64), BF),
            pltpu.VMEM((8, OWN, 256), BF),
            pltpu.VMEM((4, OWN, 2048), BF),
            pltpu.VMEM((4, OWN, 2048), BF),
            pltpu.VMEM((4, OWN, 2048), F32),
            pltpu.VMEM((3, OWN, 2048), BF),
            pltpu.VMEM((3, OWN, 2048), BF),
            dma((6,)),
            dma((6, 8)),
            dma((NB, 6)),
            dma((NB,)),
            dma((NB,)),
            dma((6, 4)),
        ],
        compiler_params=pltpu.CompilerParams(
            collective_id=0, has_side_effects=True, vmem_limit_bytes=60 * 2**20
        ),
        name="layer",
    )(
        tokens, query_down_weight, key_value_down_weight, w_rope_key, w_pool_in,
        norm_gain[None], query_latent_norm_gain[None], key_value_latent_gain[None],
        query_up_weight, key_value_up_weight, query_gain[None], key_gain[None],
        jnp.asarray(rotation_tables()), w_pool_mix, pool_scale[None], w_out_attn, w_out_pool,
    )


def solution(mesh):
    everywhere = P()
    placed = (
        (P(("sp", "tp"), None),)
        + (everywhere,) * 7
        + (P(None, "tp"),) * 2
        + (everywhere,) * 2
        + (P("tp", None, None), P("tp"), P("tp", None), P("tp", None))
    )
    return jax.shard_map(
        shards,
        mesh=mesh,
        in_specs=placed,
        out_specs=(P(("sp", "tp"), None), P("tp", "sp")),
        check_vma=False,
    )
```

```python
import numpy as np

import jax
import jax.numpy as jnp
from jax import lax
from jax.experimental import pallas as pl
from jax.experimental.pallas import tpu as pltpu
from jax.sharding import PartitionSpec as P

MESH = pl.DeviceIdType.MESH
BF, F32 = jnp.bfloat16, jnp.float32
H = 3
TB = 384
OWN = 48
NB = 32
LH = 160
PER = 4
STEPS = NB // PER
EPS = 1e-6
LOG2E = 1.4426950408889634
LN2 = 0.6931471805599453
LENGTH = NB * TB

ORDER = (
    (0, 0), (0, 1), (-1, 0), (1, 0),
    (2, 0), (0, 3), (-1, 3), (-2, 0),
    (1, 1), (1, 3), (0, 2), (-1, 1),
    (2, 3), (-1, 2), (-3, 0), (3, 0),
    (1, 2), (-2, 1), (2, 1), (-2, 3),
    (-2, 2), (3, 3), (3, 1), (4, 0),
    (-3, 3), (-3, 1), (2, 2), (4, 3),
    (-3, 2), (4, 2), (4, 1), (3, 2),
)
NEAR = ((1, 0), (-1, 0), (0, 1), (0, -1))


def slot_of(dz, dx):
    return ORDER.index(((dz + 3) % 8 - 3, dx % 4))


def forwards(core, dz, dx):
    if core == 0:
        if dz == 0:
            return {0: NEAR, 3: ((0, 1), (1, 0), (-1, 0))}.get(dx, ((1, 0), (-1, 0)))
        if dz in (-1, -2) or (dz == -3 and dx in (0, 1)):
            return ((1, 0),)
        if dz in (1, 2) or (dz == 3 and dx in (2, 3)):
            return ((-1, 0),)
        return ()
    if dx == 0:
        if dz == 0:
            return NEAR
        along = ((1, 0),) if dz in (-1, -2, -3) else ((-1, 0),) if dz in (1, 2) else ()
        return along + ((0, 1), (0, -1))
    if dx == (3 if dz % 2 == 0 else 1):
        return ((0, 1 if dx == 3 else -1),)
    return ()


PLAN = tuple(
    {
        slot_of(dz, dx): tuple((az, ax, slot_of(dz - az, dx - ax)) for az, ax in forwards(core, dz, dx))
        for dz, dx in ORDER
    }
    for core in (0, 1)
)
SERVICE = (
    ((2, 3, 5, 1), (), (), (7, 4, 10, 6, 9), (), (11, 8), (), (14, 15), (13, 16), (19, 12), (), (18,), (17,),
     (26, 23), (21,), (20, 22), (24,), (25, 31), (27,), (28,), (), (30, 29), (), ()),
    ((2, 3, 5, 1), (), (), (11, 7, 4, 6, 8, 9), (10, 13), (19, 17), (14, 15, 12), (18,), (16,), (20,), (25, 24),
     (23, 22, 21), (), (26,), (), (28, 27), (30,), (31,), (), (29,), (), (), (), ()),
)


def dot(a, b, dims):
    return lax.dot_general(a, b, (dims, ((), ())), preferred_element_type=F32)


def remote(src, dst, send, recv, device):
    return pltpu.make_async_remote_copy(
        src_ref=src, dst_ref=dst, send_sem=send, recv_sem=recv, device_id=device, device_id_type=MESH
    )


def norm_rows(v, gain):
    return v * lax.rsqrt(jnp.mean(v * v, axis=-1, keepdims=True) + EPS) * gain


def in_a_row(ref):
    v = ref[...].astype(F32)
    return jnp.concatenate([v[i : i + 1] for i in range(v.shape[0])], axis=1)


def column(row, count):
    n = row.shape[1]
    row = jnp.concatenate([row, jnp.zeros((1, 128 - n), F32)], axis=1)
    return jnp.tile(jnp.transpose(jnp.broadcast_to(row, (128, 128)))[:n], (1, count))


def prep(lat, w_ref, k_ref, v_ref, first):
    n = lat.shape[1]
    cols = slice(first, first + n)
    kv = dot(w_ref[...], lat[:256], ((1,), (0,)))
    rope = lat[256:288].astype(F32)
    rho = lat[288:304].astype(F32)
    rho = rho[0:1] + rho[1:2]
    for h in range(H):
        k = kv[h * 64 : (h + 1) * 64]
        r = lax.rsqrt((jnp.sum(k * k, axis=0, keepdims=True) + rho) * (1.0 / 96) + EPS)
        k_ref[h, 0:64, cols] = (k * r).astype(BF)
        k_ref[h, 64:96, cols] = (rope * r).astype(BF)
        v_ref[h, 0:64, cols] = kv[192 + h * 64 : 256 + h * 64].astype(BF)


def soften(h, s, m_ref, acc, v_ref):
    m_old = m_ref[h]
    m_new = jnp.maximum(m_old, jnp.broadcast_to(jnp.max(s, axis=1, keepdims=True), m_old.shape))
    m_ref[h] = m_new
    p = jnp.exp2(s - jnp.tile(m_new, (1, s.shape[1] // 128))).astype(BF)
    acc[h] = acc[h] * jnp.exp2(m_old - m_new) + dot(p, v_ref[h], ((1,), (1,)))


def layer(
    tok, h_wq, h_wkv, h_wr, h_wp, n_gain, q_gain, kv_gain, wq_up, wkv_up, hq_gain, hk_gain, tables,
    w_mix, p_scale, h_woa, h_wop,
    out, lse_out,
    w_q, w_kv, w_r, w_p, w_o, kvg, qg, psend, pool, halo, lat, qs, wup, k_ref, v_ref, m_ref, acc,
    pool_out, cat, pair_s, pair_r, own, row_s, row_r,
    w_sem, g_sem, lat_send, lat_recv, pair_recv, t_sem,
):
    sp, tp = lax.axis_index("sp"), lax.axis_index("tp")
    z, x = lax.div(sp, 4), lax.rem(sp, 4)
    y, c = lax.div(tp, 2), lax.rem(tp, 2)
    partner = tp + 1 - 2 * c

    def chip(az, ax):
        return lax.rem(z + az + 8, 8) * 4 + lax.rem(x + ax + 4, 4)

    weights = [
        pltpu.make_async_copy(a, b, w_sem.at[i])
        for i, (a, b) in enumerate(
            (
                (h_wkv, w_kv),
                (h_wr, w_r),
                (h_wq, w_q),
                (h_wp, w_p),
                (h_woa, w_o.at[pl.ds(0, 192)]),
                (h_wop, w_o.at[pl.ds(192, 64)]),
            )
        )
    ]
    for copy in weights:
        copy.start()

    barrier = pltpu.get_barrier_semaphore()
    friends = [(sp, lax.rem(tp + k, 8)) for k in range(1, 8)]
    friends += [(chip(az, ax), tp) for az, ax in NEAR]
    friends += [(lax.rem(sp + 1, NB), tp), (lax.rem(sp + NB - 1, NB), tp)]
    for friend in friends:
        pl.semaphore_signal(barrier, inc=1, device_id=friend, device_id_type=MESH)

    normed = norm_rows(tok[...].astype(F32), in_a_row(n_gain)).astype(BF)
    weights[0].wait()
    weights[1].wait()
    kv = norm_rows(dot(normed, w_kv[...], ((1,), (0,))), in_a_row(kv_gain))
    rope = dot(normed, w_r[...], ((1,), (1,)))
    kvg[tp] = jnp.concatenate([kv, rope, jnp.zeros((OWN, 96), F32)], axis=1).astype(BF)
    pl.semaphore_wait(barrier, len(friends))

    def spread(src, dst, kind):
        copies = []
        for k in (4, 3, 5, 2, 6, 1, 7):
            peer = lax.rem(tp + k, 8)
            copies.append(remote(src(peer), dst.at[tp], g_sem.at[kind, k], g_sem.at[kind + 1, 8 - k], (sp, peer)))
            copies[-1].start()
        return copies

    def gathered(dst, kind):
        for k in range(1, 8):
            peer = lax.rem(tp + k, 8)
            remote(dst.at[peer], dst.at[peer], g_sem.at[kind, k], g_sem.at[kind + 1, k], (sp, peer)).wait_recv()

    gathers = spread(lambda peer: kvg.at[tp], kvg, 0)
    weights[2].wait()
    qg[tp] = norm_rows(dot(normed, w_q[...], ((1,), (0,))), in_a_row(q_gain)).astype(BF)
    gathers += spread(lambda peer: qg.at[tp], qg, 2)
    weights[3].wait()
    pooled_in = dot(normed, w_p[...], ((1,), (0,))).astype(BF)
    for g in range(8):
        psend[g] = jnp.concatenate([pooled_in[:, g * 64 : (g + 1) * 64], jnp.zeros((OWN, 64), BF)], axis=1)
    pool[tp] = psend[tp]
    gathers += spread(lambda peer: psend.at[peer], pool, 4)

    up = jnp.transpose(wkv_up[...].astype(F32))
    for h in range(H):
        wup[h * 64 : (h + 1) * 64] = up[h * 128 : h * 128 + 64].astype(BF)
        wup[192 + h * 64 : 256 + h * 64] = up[h * 128 + 64 : h * 128 + 128].astype(BF)
    lanes = lax.broadcasted_iota(jnp.int32, (16, TB), 1)
    off_c = jnp.sum(jnp.where(lanes == sp, tables[2], 0.0), axis=1, keepdims=True)
    off_s = jnp.sum(jnp.where(lanes == sp, tables[3], 0.0), axis=1, keepdims=True)
    cosine = tables[0] * off_c - tables[1] * off_s
    sine = tables[1] * off_c + tables[0] * off_s
    kcol = column(hk_gain[...].astype(F32), 3)
    qcol = column(hq_gain[...].astype(F32), 3)
    m_ref[...] = jnp.full(m_ref.shape, -1e30, F32)
    acc[...] = jnp.zeros(acc.shape, F32)
    k_ref[...] = jnp.zeros(k_ref.shape, BF)
    v_ref[...] = jnp.zeros(v_ref.shape, BF)
    v_ref[:, 64:80, :] = jnp.ones((H, 16, v_ref.shape[2]), BF)

    gathered(kvg, 0)
    turned = jnp.transpose(kvg[...].reshape(TB, TB).astype(F32))
    rope = turned[256:288]
    rho = jnp.sum(rope * rope, axis=0, keepdims=True)
    rho_hi = rho.astype(BF).astype(F32)
    rope = rope * kcol[64:96]
    first, second = rope[:16], rope[16:]
    row = lax.broadcasted_iota(jnp.int32, (32, TB), 0)
    last = jnp.where(row == 0, rho_hi, jnp.where(row == 1, rho - rho_hi, 0.0))
    lat[0, 0] = turned[:LH].astype(BF)
    lat[0, 1] = jnp.concatenate(
        [turned[LH:256], first * cosine - second * sine, first * sine + second * cosine, last], axis=0
    ).astype(BF)

    def outgoing(core, s):
        copies = [
            remote(lat.at[s, core], lat.at[t, core], lat_send.at[s, k], lat_recv.at[t], (chip(az, ax), tp))
            for k, (az, ax, t) in enumerate(PLAN[core][s])
        ]
        if s:
            copies.append(
                remote(lat.at[s, core], lat.at[s, core], lat_send.at[s, 5], pair_recv.at[s], (sp, partner))
            )
        return copies

    def serve(point):
        for core in (0, 1):
            slots = SERVICE[core][point]
            if slots:

                @pl.when(c == core)
                def _():
                    for s in slots:
                        if s:
                            remote(
                                lat.at[s, core], lat.at[s, core], lat_send.at[s, 0], lat_recv.at[s], (sp, partner)
                            ).wait_recv()
                        for copy in outgoing(core, s):
                            copy.start()

    for core in (0, 1):

        @pl.when(c == core)
        def _():
            for copy in outgoing(core, 0):
                copy.start()

    gathered(pool, 4)
    halos = [
        remote(
            pool.at[7, pl.ds(32, 16)], halo.at[0], t_sem.at[0, 0], t_sem.at[1, 0], (lax.rem(sp + 1, NB), tp)
        ),
        remote(
            pool.at[0, pl.ds(0, 16)], halo.at[1], t_sem.at[0, 1], t_sem.at[1, 1], (lax.rem(sp + NB - 1, NB), tp)
        ),
    ]
    for copy in halos:
        copy.start()

    gathered(qg, 2)
    qt = dot(wq_up[...], qg[...].reshape(TB, 512), ((1,), (1,)))
    scale = 96.0 ** -0.5 * LOG2E
    for h in range(H):
        q = qt[h * 96 : (h + 1) * 96]
        q = q * (lax.rsqrt(jnp.mean(q * q, axis=0, keepdims=True) + EPS) * scale) * qcol
        first, second = q[64:80], q[80:96]
        q = jnp.concatenate(
            [
                q[:64] * kcol[:64],
                first * cosine - second * sine,
                first * sine + second * cosine,
                jnp.zeros((32, TB), F32),
            ],
            axis=0,
        )
        qs[h] = jnp.transpose(q).astype(BF)

    for copy in halos:
        copy.wait_recv()
    mine = pool[...].reshape(TB, 128)
    wide = jnp.concatenate([halo[0], mine, halo[1], jnp.zeros((96, 128), BF)], axis=0)
    half = jnp.left_shift(jnp.int32(1), lax.rem(tp, 4))
    here = lax.broadcasted_iota(jnp.int32, (TB, 512), 0)
    there = lax.broadcasted_iota(jnp.int32, (TB, 512), 1) - 16
    place = there + sp * TB
    band = (there >= here - half) & (there < here + half) & (place >= 0) & (place < LENGTH)
    summed = dot(jnp.where(band, 1.0, 0.0).astype(BF), wide, ((1,), (0,)))
    place = lax.broadcasted_iota(jnp.int32, (TB, 128), 0) + sp * TB
    count = jnp.minimum(place + half, LENGTH) - jnp.maximum(place - half, 0)
    pooled = (summed / count.astype(F32) - mine.astype(F32)).astype(BF)
    mapped = dot(pooled[:, :64], w_mix[0], ((1,), (0,)))
    pool_out[...] = (mapped * p_scale[...].astype(F32)).astype(BF)

    def step(i, carry):
        for k in range(STEPS):

            @pl.when(i == k)
            def _():
                if k:
                    serve(3 * k)
                else:
                    for core in (0, 1):

                        @pl.when(c == core)
                        def _():
                            for s in SERVICE[core][0]:
                                if s:
                                    remote(
                                        lat.at[s, core],
                                        lat.at[s, core],
                                        lat_send.at[s, 0],
                                        lat_recv.at[s],
                                        (sp, partner),
                                    ).wait_recv()
                                    for copy in outgoing(core, s):
                                        copy.start()

                for s in range(PER * k, PER * k + PER):
                    if s:
                        remote(
                            lat.at[s, 1 - c], lat.at[s, 1 - c], lat_send.at[s, 5], pair_recv.at[s], (sp, partner)
                        ).wait_recv()

        for j in range(PER):
            prep(lat[i * PER + j].reshape(2 * LH, TB), wup, k_ref, v_ref, j * TB)
        held = None
        for h in range(H):
            s = dot(qs[h], k_ref[h], ((1,), (0,)))
            if held is not None:
                soften(h - 1, held, m_ref, acc, v_ref)
            held = s
            if h < H - 1:
                for k in range(STEPS):
                    if any(SERVICE[core][3 * k + h + 1] for core in (0, 1)):

                        @pl.when(i == k)
                        def _():
                            serve(3 * k + h + 1)

        soften(H - 1, held, m_ref, acc, v_ref)
        return carry

    lax.fori_loop(0, STEPS, step, 0)

    lane = lax.broadcasted_iota(jnp.int32, (TB, 128), 1)
    parts, logs = [], jnp.zeros((TB, 128), F32)
    for h in range(H):
        o = acc[h]
        total = o[:, 64:65]
        parts.append((o[:, :64] / total).astype(BF))
        logs = jnp.where(lane == h, m_ref[h] * LN2 + jnp.log(total), logs)
    lse_out[...] = jnp.transpose(logs)[:H]
    cat[...] = jnp.concatenate(parts + [pool_out[...]], axis=1).reshape(8, OWN, 256)
    weights[4].wait()
    weights[5].wait()

    def rows_of(core):
        return jnp.concatenate([cat[2 * k + core] for k in range(4)], axis=0)

    pair_s[...] = dot(rows_of(1 - c), w_o[...], ((1,), (0,))).astype(BF).reshape(4, OWN, 2048)
    tails = []
    for k in (2, 1, 3, 0):
        there = lax.rem(y + k, 4)
        tails.append(
            remote(pair_s.at[there], pair_r.at[there], t_sem.at[2, k], t_sem.at[3, k], (sp, partner))
        )
        tails[-1].start()
    own[...] = dot(rows_of(c), w_o[...], ((1,), (0,))).reshape(4, OWN, 2048)
    sums = None
    for i, k in enumerate((2, 1, 3, 0)):
        there = lax.rem(y + k, 4)
        tails[i].wait_recv()
        value = own[there] + pair_r[there].astype(F32)
        if k:
            row_s[k - 1] = value.astype(BF)
            copy = remote(
                row_s.at[k - 1], row_r.at[3 - k], t_sem.at[4, k], t_sem.at[5, 4 - k], (sp, 2 * there + c)
            )
            copy.start()
            tails.append(copy)
        else:
            sums = value
    for k in (1, 3, 2):
        remote(row_s.at[k - 1], row_r.at[k - 1], t_sem.at[4, k], t_sem.at[5, k], (sp, partner)).wait_recv()
        sums = sums + row_r[k - 1].astype(F32)
    out[...] = sums.astype(BF)

    for copy in gathers + halos + tails:
        copy.wait_send()
    for core in (0, 1):

        @pl.when(c == core)
        def _():
            for s in range(NB):
                for copy in outgoing(core, s):
                    copy.wait_send()


def rotation_tables():
    half = 16
    freqs = 10000.0 ** (-np.arange(half, dtype=np.float64) / half)
    inside = freqs[:, None] * np.arange(TB)[None, :]
    blocks = np.zeros((half, TB))
    blocks[:, :NB] = freqs[:, None] * (TB * np.arange(NB))[None, :]
    return np.stack([np.cos(inside), np.sin(inside), np.cos(blocks), np.sin(blocks)]).astype(np.float32)


def shards(tokens, norm_gain, query_down_weight, query_latent_norm_gain, key_value_down_weight,
           key_value_latent_gain, w_rope_key, w_pool_in, query_up_weight, key_value_up_weight,
           query_gain, key_gain, w_pool_mix, pool_scale, w_out_attn, w_out_pool):
    vmem, anywhere = pl.BlockSpec(memory_space=pltpu.VMEM), pl.BlockSpec(memory_space=pl.ANY)
    dma, n = pltpu.SemaphoreType.DMA, PER * TB
    return pl.pallas_call(
        layer,
        out_shape=(jax.ShapeDtypeStruct((OWN, 2048), BF), jax.ShapeDtypeStruct((H, TB), F32)),
        in_specs=[vmem] + [anywhere] * 4 + [vmem] * 10 + [anywhere] * 2,
        out_specs=(vmem, vmem),
        scratch_shapes=[
            pltpu.VMEM((2048, 512), BF),
            pltpu.VMEM((2048, 256), BF),
            pltpu.VMEM((32, 2048), BF),
            pltpu.VMEM((2048, 512), BF),
            pltpu.VMEM((256, 2048), BF),
            pltpu.VMEM((8, OWN, TB), BF),
            pltpu.VMEM((8, OWN, 512), BF),
            pltpu.VMEM((8, OWN, 128), BF),
            pltpu.VMEM((8, OWN, 128), BF),
            pltpu.VMEM((2, 16, 128), BF),
            pltpu.VMEM((NB, 2, LH, TB), BF),
            pltpu.VMEM((H, TB, 128), BF),
            pltpu.VMEM((H * 128, 256), BF),
            pltpu.VMEM((H, 128, n), BF),
            pltpu.VMEM((H, 128, n), BF),
            pltpu.VMEM((H, TB, 128), F32),
            pltpu.VMEM((H, TB, 128), F32),
            pltpu.VMEM((TB, 64), BF),
            pltpu.VMEM((8, OWN, 256), BF),
            pltpu.VMEM((4, OWN, 2048), BF),
            pltpu.VMEM((4, OWN, 2048), BF),
            pltpu.VMEM((4, OWN, 2048), F32),
            pltpu.VMEM((3, OWN, 2048), BF),
            pltpu.VMEM((3, OWN, 2048), BF),
            dma((6,)),
            dma((6, 8)),
            dma((NB, 6)),
            dma((NB,)),
            dma((NB,)),
            dma((6, 4)),
        ],
        compiler_params=pltpu.CompilerParams(
            collective_id=0, has_side_effects=True, vmem_limit_bytes=60 * 2**20
        ),
        name="layer",
    )(
        tokens, query_down_weight, key_value_down_weight, w_rope_key.T, w_pool_in,
        norm_gain.reshape(16, 128), query_latent_norm_gain.reshape(4, 128), key_value_latent_gain.reshape(2, 128),
        query_up_weight.T, key_value_up_weight, query_gain[None], key_gain[None],
        jnp.asarray(rotation_tables()), w_pool_mix, pool_scale[None], w_out_attn, w_out_pool,
    )


def solution(mesh):
    everywhere = P()
    placed = (
        (P(("sp", "tp"), None),)
        + (everywhere,) * 7
        + (P(None, "tp"),) * 2
        + (everywhere,) * 2
        + (P("tp", None, None), P("tp"), P("tp", None), P("tp", None))
    )
    return jax.shard_map(
        shards,
        mesh=mesh,
        in_specs=placed,
        out_specs=(P(("sp", "tp"), None), P("tp", "sp")),
        check_vma=False,
    )
```

```python
import numpy as np

import jax
import jax.numpy as jnp
from jax import lax
from jax.experimental import pallas as pl
from jax.experimental.pallas import tpu as pltpu
from jax.sharding import PartitionSpec as P

MESH = pl.DeviceIdType.MESH
BF, F32 = jnp.bfloat16, jnp.float32
H = 3
TB = 384
OWN = 48
NB = 32
LH = 160
PER = 4
STEPS = NB // PER
EPS = 1e-6
LOG2E = 1.4426950408889634
LN2 = 0.6931471805599453
LENGTH = NB * TB

ORDER = (
    (0, 0), (0, 1), (-1, 0), (1, 0),
    (2, 0), (0, 3), (-1, 3), (-2, 0),
    (1, 1), (1, 3), (0, 2), (-1, 1),
    (2, 3), (-1, 2), (-3, 0), (3, 0),
    (1, 2), (-2, 1), (2, 1), (-2, 3),
    (-2, 2), (3, 3), (3, 1), (4, 0),
    (-3, 3), (-3, 1), (2, 2), (4, 3),
    (-3, 2), (4, 2), (4, 1), (3, 2),
)
NEAR = ((1, 0), (-1, 0), (0, 1), (0, -1))


def slot_of(dz, dx):
    return ORDER.index(((dz + 3) % 8 - 3, dx % 4))


def forwards(core, dz, dx):
    if core == 0:
        if dz == 0:
            return {0: NEAR, 3: ((0, 1), (1, 0), (-1, 0))}.get(dx, ((1, 0), (-1, 0)))
        if dz in (-1, -2) or (dz == -3 and dx in (0, 1)):
            return ((1, 0),)
        if dz in (1, 2) or (dz == 3 and dx in (2, 3)):
            return ((-1, 0),)
        return ()
    if dx == 0:
        if dz == 0:
            return NEAR
        along = ((1, 0),) if dz in (-1, -2, -3) else ((-1, 0),) if dz in (1, 2) else ()
        return along + ((0, 1), (0, -1))
    if dx == (3 if dz % 2 == 0 else 1):
        return ((0, 1 if dx == 3 else -1),)
    return ()


PLAN = tuple(
    {
        slot_of(dz, dx): tuple((az, ax, slot_of(dz - az, dx - ax)) for az, ax in forwards(core, dz, dx))
        for dz, dx in ORDER
    }
    for core in (0, 1)
)
SERVICE = (
    ((2, 3, 5, 1), (), (), (7, 4, 10, 6, 9), (), (11, 8), (), (14, 15), (13, 16), (19, 12), (), (18,), (17,),
     (26, 23), (21,), (20, 22), (24,), (25, 31), (27,), (28,), (), (30, 29), (), ()),
    ((2, 3, 5, 1), (), (), (11, 7, 4, 6, 8, 9), (10, 13), (19, 17), (14, 15, 12), (18,), (16,), (20,), (25, 24),
     (23, 22, 21), (), (26,), (), (28, 27), (30,), (31,), (), (29,), (), (), (), ()),
)


W_STEPS = {4: (0, 1), 7: (2, 3)}


def dot(a, b, dims):
    return lax.dot_general(a, b, (dims, ((), ())), preferred_element_type=F32)


def remote(src, dst, send, recv, device):
    return pltpu.make_async_remote_copy(
        src_ref=src, dst_ref=dst, send_sem=send, recv_sem=recv, device_id=device, device_id_type=MESH
    )


def norm_rows(v, gain):
    return v * lax.rsqrt(jnp.mean(v * v, axis=-1, keepdims=True) + EPS) * gain


def in_a_row(ref):
    v = ref[...].astype(F32)
    return jnp.concatenate([v[i : i + 1] for i in range(v.shape[0])], axis=1)


def column(row, count):
    n = row.shape[1]
    row = jnp.concatenate([row, jnp.zeros((1, 128 - n), F32)], axis=1)
    return jnp.tile(jnp.transpose(jnp.broadcast_to(row, (128, 128)))[:n], (1, count))


def prep(lat, w_ref, k_ref, v_ref, first):
    n = lat.shape[1]
    cols = slice(first, first + n)
    kv = dot(w_ref[...], lat[:256], ((1,), (0,)))
    rope = lat[256:288].astype(F32)
    rho = lat[288:304].astype(F32)
    rho = rho[0:1] + rho[1:2]
    for h in range(H):
        k = kv[h * 64 : (h + 1) * 64]
        r = lax.rsqrt((jnp.sum(k * k, axis=0, keepdims=True) + rho) * (1.0 / 96) + EPS)
        k_ref[h, 0:64, cols] = (k * r).astype(BF)
        k_ref[h, 64:96, cols] = (rope * r).astype(BF)
        v_ref[h, 0:64, cols] = kv[192 + h * 64 : 256 + h * 64].astype(BF)


def soften(h, s, m_ref, acc, v_ref):
    m_old = m_ref[h]
    m_new = jnp.maximum(m_old, jnp.broadcast_to(jnp.max(s, axis=1, keepdims=True), m_old.shape))
    m_ref[h] = m_new
    p = jnp.exp2(s - jnp.tile(m_new, (1, s.shape[1] // 128))).astype(BF)
    acc[h] = acc[h] * jnp.exp2(m_old - m_new) + dot(p, v_ref[h], ((1,), (1,)))


def layer(
    tok, h_wq, h_wkv, h_wr, h_wp, n_gain, q_gain, kv_gain, wq_up, wkv_up, hq_gain, hk_gain, tables,
    w_mix, p_scale, h_woa, h_wop,
    out, lse_out,
    w_q, w_kv, w_r, w_p, w_o, kvg, qg, psend, pool, halo, lat, qs, wup, k_ref, v_ref, m_ref, acc,
    pool_out, cat, cat_r,
    w_sem, g_sem, lat_send, lat_recv, pair_recv, o_send, o_recv, o_pair, t_sem,
):
    sp, tp = lax.axis_index("sp"), lax.axis_index("tp")
    z, x = lax.div(sp, 4), lax.rem(sp, 4)
    y, c = lax.div(tp, 2), lax.rem(tp, 2)
    partner = tp + 1 - 2 * c

    def chip(az, ax):
        return lax.rem(z + az + 8, 8) * 4 + lax.rem(x + ax + 4, 4)

    weights = [
        pltpu.make_async_copy(a, b, w_sem.at[i])
        for i, (a, b) in enumerate(
            (
                (h_wkv, w_kv),
                (h_wr, w_r),
                (h_wq, w_q),
                (h_wp, w_p),
                (h_woa, w_o.at[c, pl.ds(0, 192)]),
                (h_wop, w_o.at[c, pl.ds(192, 64)]),
            )
        )
    ]
    for copy in weights:
        copy.start()

    barrier = pltpu.get_barrier_semaphore()
    friends = [(sp, lax.rem(tp + k, 8)) for k in range(1, 8)]
    friends += [(chip(az, ax), tp) for az, ax in NEAR]
    friends += [(lax.rem(sp + 1, NB), tp), (lax.rem(sp + NB - 1, NB), tp)]
    for friend in friends:
        pl.semaphore_signal(barrier, inc=1, device_id=friend, device_id_type=MESH)

    normed = norm_rows(tok[...].astype(F32), in_a_row(n_gain)).astype(BF)
    weights[0].wait()
    weights[1].wait()
    kv = norm_rows(dot(normed, w_kv[...], ((1,), (0,))), in_a_row(kv_gain))
    rope = dot(normed, w_r[...], ((1,), (1,)))
    kvg[tp] = jnp.concatenate([kv, rope, jnp.zeros((OWN, 96), F32)], axis=1).astype(BF)
    pl.semaphore_wait(barrier, len(friends))

    def spread(rows, kind):
        copies = []
        for k in (2, 1, 3):
            peer = 2 * lax.rem(y + k, 4) + c
            copies.append(remote(rows.at[tp], rows.at[tp], g_sem.at[kind, k], g_sem.at[kind + 1, 4 - k], (sp, peer)))
        copies.append(remote(rows.at[tp], rows.at[tp], g_sem.at[kind, 4], g_sem.at[kind + 1, 4], (sp, partner)))
        for copy in copies:
            copy.start()
        return copies

    def gathered(rows, kind):
        copies = []
        for k in (1, 3, 2):
            peer = 2 * lax.rem(y + k, 4) + c
            remote(rows.at[peer], rows.at[peer], g_sem.at[kind, k], g_sem.at[kind + 1, k], (sp, peer)).wait_recv()
            copies.append(
                remote(rows.at[peer], rows.at[peer], g_sem.at[kind, 4 + k], g_sem.at[kind + 1, 4 + k], (sp, partner))
            )
            copies[-1].start()
        for k in (0, 1, 3, 2):
            peer = 2 * lax.rem(y + k, 4) + 1 - c
            remote(
                rows.at[peer], rows.at[peer], g_sem.at[kind, 4 + k], g_sem.at[kind + 1, 4 + k], (sp, partner)
            ).wait_recv()
        return copies

    gathers = spread(kvg, 0)
    weights[2].wait()
    qg[tp] = norm_rows(dot(normed, w_q[...], ((1,), (0,))), in_a_row(q_gain)).astype(BF)
    gathers += spread(qg, 2)
    weights[3].wait()
    pooled_in = dot(normed, w_p[...], ((1,), (0,))).astype(BF)
    for g in range(8):
        psend[g] = jnp.concatenate([pooled_in[:, g * 64 : (g + 1) * 64], jnp.zeros((OWN, 64), BF)], axis=1)
    pool[tp] = psend[tp]

    def exchange(src, dst, kind):
        copies = []
        for k in (4, 3, 5, 2, 6, 7, 1):
            peer = lax.rem(tp + k, 8)
            copies.append(
                remote(src.at[peer], dst.at[tp], g_sem.at[kind, k], g_sem.at[kind + 1, 8 - k], (sp, peer))
            )
            copies[-1].start()
        return copies

    def exchanged(dst, kind, k):
        peer = lax.rem(tp + k, 8)
        remote(dst.at[peer], dst.at[peer], g_sem.at[kind, k], g_sem.at[kind + 1, k], (sp, peer)).wait_recv()

    gathers += exchange(psend, pool, 4)

    weights[4].wait()
    weights[5].wait()

    def half_of(shard, part):
        return w_o.at[shard, pl.ds(128 * part, 128)]

    def around(k, part, i, step):
        return remote(
            half_of(2 * k + c, part),
            half_of(2 * ((k - step) % 4) + c, part),
            o_send.at[i],
            o_recv.at[i],
            (sp, 2 * lax.rem(y + step + 4, 4) + c),
        )

    def across(k, part):
        shard = half_of(2 * k + c, part)
        return remote(shard, shard, o_send.at[6 + 2 * k + part], o_pair.at[2 * k + part], (sp, partner))

    rounds = [around(0, 1, 0, 1), around(0, 0, 1, -1), around(0, 0, 2, 1), around(0, 1, 3, -1)]
    rounds += [around(3, 1, 4, 1), around(1, 0, 5, -1)]
    landed = ((3, 1), (1, 0), (3, 0), (1, 1), (2, 1), (2, 0))
    acrosses = {(k, part): across(k, part) for k in range(4) for part in (0, 1)}
    for copy in rounds[:4]:
        copy.start()
    acrosses[0, 0].start()
    acrosses[0, 1].start()

    def pass_on(i):
        rounds[i].wait_recv()
        if i < 2:
            rounds[4 + i].start()
        acrosses[landed[i]].start()

    up = jnp.transpose(wkv_up[...].astype(F32))
    for h in range(H):
        wup[h * 64 : (h + 1) * 64] = up[h * 128 : h * 128 + 64].astype(BF)
        wup[192 + h * 64 : 256 + h * 64] = up[h * 128 + 64 : h * 128 + 128].astype(BF)
    lanes = lax.broadcasted_iota(jnp.int32, (16, TB), 1)
    off_c = jnp.sum(jnp.where(lanes == sp, tables[2], 0.0), axis=1, keepdims=True)
    off_s = jnp.sum(jnp.where(lanes == sp, tables[3], 0.0), axis=1, keepdims=True)
    cosine = tables[0] * off_c - tables[1] * off_s
    sine = tables[1] * off_c + tables[0] * off_s
    kcol = column(hk_gain[...].astype(F32), 3)
    qcol = column(hq_gain[...].astype(F32), 3)
    m_ref[...] = jnp.full(m_ref.shape, -1e30, F32)
    acc[...] = jnp.zeros(acc.shape, F32)
    k_ref[...] = jnp.zeros(k_ref.shape, BF)
    v_ref[...] = jnp.zeros(v_ref.shape, BF)
    v_ref[:, 64:80, :] = jnp.ones((H, 16, v_ref.shape[2]), BF)

    gathers += gathered(kvg, 0)
    turned = jnp.transpose(kvg[...].reshape(TB, TB).astype(F32))
    rope = turned[256:288]
    rho = jnp.sum(rope * rope, axis=0, keepdims=True)
    rho_hi = rho.astype(BF).astype(F32)
    rope = rope * kcol[64:96]
    first, second = rope[:16], rope[16:]
    row = lax.broadcasted_iota(jnp.int32, (32, TB), 0)
    last = jnp.where(row == 0, rho_hi, jnp.where(row == 1, rho - rho_hi, 0.0))
    lat[0, 0] = turned[:LH].astype(BF)
    lat[0, 1] = jnp.concatenate(
        [turned[LH:256], first * cosine - second * sine, first * sine + second * cosine, last], axis=0
    ).astype(BF)

    def outgoing(core, s):
        copies = [
            remote(lat.at[s, core], lat.at[t, core], lat_send.at[s, k], lat_recv.at[t], (chip(az, ax), tp))
            for k, (az, ax, t) in enumerate(PLAN[core][s])
        ]
        if s:
            copies.append(
                remote(lat.at[s, core], lat.at[s, core], lat_send.at[s, 5], pair_recv.at[s], (sp, partner))
            )
        return copies

    def serve(point):
        for core in (0, 1):
            slots = SERVICE[core][point]
            if slots:

                @pl.when(c == core)
                def _():
                    for s in slots:
                        if s:
                            remote(
                                lat.at[s, core], lat.at[s, core], lat_send.at[s, 0], lat_recv.at[s], (sp, partner)
                            ).wait_recv()
                        for copy in outgoing(core, s):
                            copy.start()

    for core in (0, 1):

        @pl.when(c == core)
        def _():
            for copy in outgoing(core, 0):
                copy.start()

    gathers += gathered(qg, 2)
    qt = dot(wq_up[...], qg[...].reshape(TB, 512), ((1,), (1,)))
    scale = 96.0 ** -0.5 * LOG2E
    for h in range(H):
        q = qt[h * 96 : (h + 1) * 96]
        q = q * (lax.rsqrt(jnp.mean(q * q, axis=0, keepdims=True) + EPS) * scale) * qcol
        first, second = q[64:80], q[80:96]
        q = jnp.concatenate(
            [
                q[:64] * kcol[:64],
                first * cosine - second * sine,
                first * sine + second * cosine,
                jnp.zeros((32, TB), F32),
            ],
            axis=0,
        )
        qs[h] = jnp.transpose(q).astype(BF)

    for k in range(1, 8):
        exchanged(pool, 4, k)
    halos = [
        remote(
            pool.at[7, pl.ds(32, 16)], halo.at[0], t_sem.at[0, 0], t_sem.at[1, 0], (lax.rem(sp + 1, NB), tp)
        ),
        remote(
            pool.at[0, pl.ds(0, 16)], halo.at[1], t_sem.at[0, 1], t_sem.at[1, 1], (lax.rem(sp + NB - 1, NB), tp)
        ),
    ]
    for copy in halos:
        copy.start()

    def pooling():
        for copy in halos:
            copy.wait_recv()
        mine = pool[...].reshape(TB, 128)
        wide = jnp.concatenate([halo[0], mine, halo[1], jnp.zeros((96, 128), BF)], axis=0)
        half = jnp.left_shift(jnp.int32(1), lax.rem(tp, 4))
        here = lax.broadcasted_iota(jnp.int32, (TB, 512), 0)
        there = lax.broadcasted_iota(jnp.int32, (TB, 512), 1) - 16
        place = there + sp * TB
        band = (there >= here - half) & (there < here + half) & (place >= 0) & (place < LENGTH)
        summed = dot(jnp.where(band, 1.0, 0.0).astype(BF), wide, ((1,), (0,)))
        place = lax.broadcasted_iota(jnp.int32, (TB, 128), 0) + sp * TB
        count = jnp.minimum(place + half, LENGTH) - jnp.maximum(place - half, 0)
        pooled = (summed / count.astype(F32) - mine.astype(F32)).astype(BF)
        mapped = dot(pooled[:, :64], w_mix[0], ((1,), (0,)))
        pool_out[...] = (mapped * p_scale[...].astype(F32)).astype(BF)

    def step(i, carry):
        for k in range(STEPS):

            @pl.when(i == k)
            def _():
                if k == 1:
                    pooling()
                for i_round in W_STEPS.get(k, ()):
                    pass_on(i_round)
                if k:
                    serve(3 * k)
                else:
                    for core in (0, 1):

                        @pl.when(c == core)
                        def _():
                            for s in SERVICE[core][0]:
                                if s:
                                    remote(
                                        lat.at[s, core],
                                        lat.at[s, core],
                                        lat_send.at[s, 0],
                                        lat_recv.at[s],
                                        (sp, partner),
                                    ).wait_recv()
                                    for copy in outgoing(core, s):
                                        copy.start()

                for s in range(PER * k, PER * k + PER):
                    if s:
                        remote(
                            lat.at[s, 1 - c], lat.at[s, 1 - c], lat_send.at[s, 5], pair_recv.at[s], (sp, partner)
                        ).wait_recv()

        for j in range(PER):
            prep(lat[i * PER + j].reshape(2 * LH, TB), wup, k_ref, v_ref, j * TB)
        held = None
        for h in range(H):
            s = dot(qs[h], k_ref[h], ((1,), (0,)))
            if held is not None:
                soften(h - 1, held, m_ref, acc, v_ref)
            held = s
            if h < H - 1:
                for k in range(STEPS):
                    if any(SERVICE[core][3 * k + h + 1] for core in (0, 1)):

                        @pl.when(i == k)
                        def _():
                            serve(3 * k + h + 1)

        soften(H - 1, held, m_ref, acc, v_ref)
        return carry

    lax.fori_loop(0, STEPS, step, 0)

    lane = lax.broadcasted_iota(jnp.int32, (TB, 128), 1)
    parts, logs = [], jnp.zeros((TB, 128), F32)
    for h in range(H):
        o = acc[h]
        total = o[:, 64:65]
        parts.append((o[:, :64] / total).astype(BF))
        logs = jnp.where(lane == h, m_ref[h] * LN2 + jnp.log(total), logs)
    lse_out[...] = jnp.transpose(logs)[:H]
    cat[...] = jnp.concatenate(parts + [pool_out[...]], axis=1).reshape(8, OWN, 256)
    tails = exchange(cat, cat_r, 6)
    sums = dot(cat[tp], w_o[c], ((1,), (0,)))
    pass_on(4)
    pass_on(5)
    for k in (0, 1, 3, 2):
        for core in (1 - c, c):
            if k == 0 and core is c:
                continue
            member = 2 * lax.rem(y + k, 4) + core
            if core is not c:
                for part in (0, 1):
                    acrosses[k, part].wait_recv()
            away = lax.rem(member - tp + 8, 8)
            remote(
                cat_r.at[member], cat_r.at[member], g_sem.at[6, away], g_sem.at[7, away], (sp, partner)
            ).wait_recv()
            sums = sums + dot(cat_r[member], w_o[2 * k + core], ((1,), (0,)))
    out[...] = sums.astype(BF)

    for copy in gathers + halos + tails + rounds + list(acrosses.values()):
        copy.wait_send()
    for core in (0, 1):

        @pl.when(c == core)
        def _():
            for s in range(NB):
                for copy in outgoing(core, s):
                    copy.wait_send()


def rotation_tables():
    half = 16
    freqs = 10000.0 ** (-np.arange(half, dtype=np.float64) / half)
    inside = freqs[:, None] * np.arange(TB)[None, :]
    blocks = np.zeros((half, TB))
    blocks[:, :NB] = freqs[:, None] * (TB * np.arange(NB))[None, :]
    return np.stack([np.cos(inside), np.sin(inside), np.cos(blocks), np.sin(blocks)]).astype(np.float32)


def shards(tokens, norm_gain, query_down_weight, query_latent_norm_gain, key_value_down_weight,
           key_value_latent_gain, w_rope_key, w_pool_in, query_up_weight, key_value_up_weight,
           query_gain, key_gain, w_pool_mix, pool_scale, w_out_attn, w_out_pool):
    vmem, anywhere = pl.BlockSpec(memory_space=pltpu.VMEM), pl.BlockSpec(memory_space=pl.ANY)
    dma, n = pltpu.SemaphoreType.DMA, PER * TB
    return pl.pallas_call(
        layer,
        out_shape=(jax.ShapeDtypeStruct((OWN, 2048), BF), jax.ShapeDtypeStruct((H, TB), F32)),
        in_specs=[vmem] + [anywhere] * 4 + [vmem] * 10 + [anywhere] * 2,
        out_specs=(vmem, vmem),
        scratch_shapes=[
            pltpu.VMEM((2048, 512), BF),
            pltpu.VMEM((2048, 256), BF),
            pltpu.VMEM((32, 2048), BF),
            pltpu.VMEM((2048, 512), BF),
            pltpu.VMEM((8, 256, 2048), BF),
            pltpu.VMEM((8, OWN, TB), BF),
            pltpu.VMEM((8, OWN, 512), BF),
            pltpu.VMEM((8, OWN, 128), BF),
            pltpu.VMEM((8, OWN, 128), BF),
            pltpu.VMEM((2, 16, 128), BF),
            pltpu.VMEM((NB, 2, LH, TB), BF),
            pltpu.VMEM((H, TB, 128), BF),
            pltpu.VMEM((H * 128, 256), BF),
            pltpu.VMEM((H, 128, n), BF),
            pltpu.VMEM((H, 128, n), BF),
            pltpu.VMEM((H, TB, 128), F32),
            pltpu.VMEM((H, TB, 128), F32),
            pltpu.VMEM((TB, 64), BF),
            pltpu.VMEM((8, OWN, 256), BF),
            pltpu.VMEM((8, OWN, 256), BF),
            dma((6,)),
            dma((8, 8)),
            dma((NB, 6)),
            dma((NB,)),
            dma((NB,)),
            dma((14,)),
            dma((6,)),
            dma((8,)),
            dma((2, 2)),
        ],
        compiler_params=pltpu.CompilerParams(
            collective_id=0, has_side_effects=True, vmem_limit_bytes=60 * 2**20
        ),
        name="layer",
    )(
        tokens, query_down_weight, key_value_down_weight, w_rope_key.T, w_pool_in,
        norm_gain.reshape(16, 128), query_latent_norm_gain.reshape(4, 128), key_value_latent_gain.reshape(2, 128),
        query_up_weight.T, key_value_up_weight, query_gain[None], key_gain[None],
        jnp.asarray(rotation_tables()), w_pool_mix, pool_scale[None], w_out_attn, w_out_pool,
    )


def solution(mesh):
    everywhere = P()
    placed = (
        (P(("sp", "tp"), None),)
        + (everywhere,) * 7
        + (P(None, "tp"),) * 2
        + (everywhere,) * 2
        + (P("tp", None, None), P("tp"), P("tp", None), P("tp", None))
    )
    return jax.shard_map(
        shards,
        mesh=mesh,
        in_specs=placed,
        out_specs=(P(("sp", "tp"), None), P("tp", "sp")),
        check_vma=False,
    )
```

```python
import numpy as np

import jax
import jax.numpy as jnp
from jax import lax
from jax.experimental import pallas as pl
from jax.experimental.pallas import tpu as pltpu
from jax.sharding import PartitionSpec as P

MESH = pl.DeviceIdType.MESH
BF, F32 = jnp.bfloat16, jnp.float32
H = 3
TB = 384
OWN = 48
NB = 32
LH = 160
PER = 4
STEPS = NB // PER
EPS = 1e-6
LOG2E = 1.4426950408889634
LN2 = 0.6931471805599453
LENGTH = NB * TB

ORDER = (
    (0, 0), (0, 1), (-1, 0), (1, 0),
    (2, 0), (0, 3), (-1, 3), (-2, 0),
    (1, 1), (1, 3), (0, 2), (-1, 1),
    (2, 3), (-1, 2), (-3, 0), (3, 0),
    (1, 2), (-2, 1), (2, 1), (-2, 3),
    (-2, 2), (3, 3), (3, 1), (4, 0),
    (-3, 3), (-3, 1), (2, 2), (4, 3),
    (-3, 2), (4, 2), (4, 1), (3, 2),
)
NEAR = ((1, 0), (-1, 0), (0, 1), (0, -1))


def slot_of(dz, dx):
    return ORDER.index(((dz + 3) % 8 - 3, dx % 4))


def forwards(core, dz, dx):
    if core == 0:
        if dz == 0:
            return {0: NEAR, 3: ((0, 1), (1, 0), (-1, 0))}.get(dx, ((1, 0), (-1, 0)))
        if dz in (-1, -2) or (dz == -3 and dx in (0, 1)):
            return ((1, 0),)
        if dz in (1, 2) or (dz == 3 and dx in (2, 3)):
            return ((-1, 0),)
        return ()
    if dx == 0:
        if dz == 0:
            return NEAR
        along = ((1, 0),) if dz in (-1, -2, -3) else ((-1, 0),) if dz in (1, 2) else ()
        return along + ((0, 1), (0, -1))
    if dx == (3 if dz % 2 == 0 else 1):
        return ((0, 1 if dx == 3 else -1),)
    return ()


PLAN = tuple(
    {
        slot_of(dz, dx): tuple((az, ax, slot_of(dz - az, dx - ax)) for az, ax in forwards(core, dz, dx))
        for dz, dx in ORDER
    }
    for core in (0, 1)
)
SERVICE = (
    ((2, 3, 5, 1), (), (), (7, 4, 10, 6, 9), (), (11, 8), (), (14, 15), (13, 16), (19, 12), (), (18,), (17,),
     (26, 23), (21,), (20, 22), (24,), (25, 31), (27,), (28,), (), (30, 29), (), ()),
    ((2, 3, 5, 1), (), (), (11, 7, 4, 6, 8, 9), (10, 13), (19, 17), (14, 15, 12), (18,), (16,), (20,), (25, 24),
     (23, 22, 21), (), (26,), (), (28, 27), (30,), (31,), (), (29,), (), (), (), ()),
)


W_STEPS = {4: (0, 1), 7: (2, 3)}


def dot(a, b, dims):
    return lax.dot_general(a, b, (dims, ((), ())), preferred_element_type=F32)


def remote(src, dst, send, recv, device):
    return pltpu.make_async_remote_copy(
        src_ref=src, dst_ref=dst, send_sem=send, recv_sem=recv, device_id=device, device_id_type=MESH
    )


def norm_rows(v, gain):
    return v * lax.rsqrt(jnp.mean(v * v, axis=-1, keepdims=True) + EPS) * gain


def in_a_row(ref):
    v = ref[...].astype(F32)
    return jnp.concatenate([v[i : i + 1] for i in range(v.shape[0])], axis=1)


def column(row, count):
    n = row.shape[1]
    row = jnp.concatenate([row, jnp.zeros((1, 128 - n), F32)], axis=1)
    return jnp.tile(jnp.transpose(jnp.broadcast_to(row, (128, 128)))[:n], (1, count))


def prep(lat, w_ref, k_ref, v_ref, first):
    n = lat.shape[1]
    cols = slice(first, first + n)
    kv = dot(w_ref[...], lat[:256], ((1,), (0,)))
    rope = lat[256:288].astype(F32)
    rho = lat[288:304].astype(F32)
    rho = rho[0:1] + rho[1:2]
    for h in range(H):
        k = kv[h * 64 : (h + 1) * 64]
        r = lax.rsqrt((jnp.sum(k * k, axis=0, keepdims=True) + rho) * (1.0 / 96) + EPS)
        k_ref[h, 0:64, cols] = (k * r).astype(BF)
        k_ref[h, 64:96, cols] = (rope * r).astype(BF)
        v_ref[h, 0:64, cols] = kv[192 + h * 64 : 256 + h * 64].astype(BF)


def soften(h, s, m_ref, acc, v_ref):
    m_old = m_ref[h]
    m_new = jnp.maximum(m_old, jnp.broadcast_to(jnp.max(s, axis=1, keepdims=True), m_old.shape))
    m_ref[h] = m_new
    p = jnp.exp2(s - jnp.tile(m_new, (1, s.shape[1] // 128))).astype(BF)
    acc[h] = acc[h] * jnp.exp2(m_old - m_new) + dot(p, v_ref[h], ((1,), (1,)))


def layer(
    tok, h_wq, h_wkv, h_wr, h_wp, n_gain, q_gain, kv_gain, wq_up, wkv_up, hq_gain, hk_gain, tables,
    w_mix, p_scale, h_woa, h_wop,
    out, lse_out,
    w_q, w_kv, w_r, w_p, w_o, kvg, qg, psend, pool, halo, lat, qs, wup, k_ref, v_ref, m_ref, acc,
    s_ref, pool_out, cat, cat_r,
    w_sem, g_sem, lat_send, lat_recv, pair_recv, o_send, o_recv, o_pair, t_sem,
):
    sp, tp = lax.axis_index("sp"), lax.axis_index("tp")
    z, x = lax.div(sp, 4), lax.rem(sp, 4)
    y, c = lax.div(tp, 2), lax.rem(tp, 2)
    partner = tp + 1 - 2 * c

    def chip(az, ax):
        return lax.rem(z + az + 8, 8) * 4 + lax.rem(x + ax + 4, 4)

    weights = [
        pltpu.make_async_copy(a, b, w_sem.at[i])
        for i, (a, b) in enumerate(
            (
                (h_wkv, w_kv),
                (h_wr, w_r),
                (h_wq, w_q),
                (h_wp, w_p),
                (h_woa, w_o.at[c, pl.ds(0, 192)]),
                (h_wop, w_o.at[c, pl.ds(192, 64)]),
            )
        )
    ]
    for copy in weights:
        copy.start()

    barrier = pltpu.get_barrier_semaphore()
    friends = [(sp, lax.rem(tp + k, 8)) for k in range(1, 8)]
    friends += [(chip(az, ax), tp) for az, ax in NEAR]
    friends += [(lax.rem(sp + 1, NB), tp), (lax.rem(sp + NB - 1, NB), tp)]
    for friend in friends:
        pl.semaphore_signal(barrier, inc=1, device_id=friend, device_id_type=MESH)

    normed = norm_rows(tok[...].astype(F32), in_a_row(n_gain)).astype(BF)
    weights[0].wait()
    weights[1].wait()
    kv = norm_rows(dot(normed, w_kv[...], ((1,), (0,))), in_a_row(kv_gain))
    rope = dot(normed, w_r[...], ((1,), (1,)))
    kvg[tp] = jnp.concatenate([kv, rope, jnp.zeros((OWN, 96), F32)], axis=1).astype(BF)
    pl.semaphore_wait(barrier, len(friends))

    def spread(rows, kind):
        copies = []
        for k in (2, 1, 3):
            peer = 2 * lax.rem(y + k, 4) + c
            copies.append(remote(rows.at[tp], rows.at[tp], g_sem.at[kind, k], g_sem.at[kind + 1, 4 - k], (sp, peer)))
        copies.append(remote(rows.at[tp], rows.at[tp], g_sem.at[kind, 4], g_sem.at[kind + 1, 4], (sp, partner)))
        for copy in copies:
            copy.start()
        return copies

    def gathered(rows, kind):
        copies = []
        for k in (1, 3, 2):
            peer = 2 * lax.rem(y + k, 4) + c
            remote(rows.at[peer], rows.at[peer], g_sem.at[kind, k], g_sem.at[kind + 1, k], (sp, peer)).wait_recv()
            copies.append(
                remote(rows.at[peer], rows.at[peer], g_sem.at[kind, 4 + k], g_sem.at[kind + 1, 4 + k], (sp, partner))
            )
            copies[-1].start()
        for k in (0, 1, 3, 2):
            peer = 2 * lax.rem(y + k, 4) + 1 - c
            remote(
                rows.at[peer], rows.at[peer], g_sem.at[kind, 4 + k], g_sem.at[kind + 1, 4 + k], (sp, partner)
            ).wait_recv()
        return copies

    gathers = spread(kvg, 0)
    weights[2].wait()
    qg[tp] = norm_rows(dot(normed, w_q[...], ((1,), (0,))), in_a_row(q_gain)).astype(BF)
    gathers += spread(qg, 2)
    weights[3].wait()
    pooled_in = dot(normed, w_p[...], ((1,), (0,))).astype(BF)
    for g in range(8):
        psend[g] = jnp.concatenate([pooled_in[:, g * 64 : (g + 1) * 64], jnp.zeros((OWN, 64), BF)], axis=1)
    pool[tp] = psend[tp]

    def exchange(src, dst, kind):
        copies = []
        for k in (4, 3, 5, 2, 6, 7, 1):
            peer = lax.rem(tp + k, 8)
            copies.append(
                remote(src.at[peer], dst.at[tp], g_sem.at[kind, k], g_sem.at[kind + 1, 8 - k], (sp, peer))
            )
            copies[-1].start()
        return copies

    def exchanged(dst, kind, k):
        peer = lax.rem(tp + k, 8)
        remote(dst.at[peer], dst.at[peer], g_sem.at[kind, k], g_sem.at[kind + 1, k], (sp, peer)).wait_recv()

    gathers += exchange(psend, pool, 4)

    weights[4].wait()
    weights[5].wait()

    def half_of(shard, part):
        return w_o.at[shard, pl.ds(128 * part, 128)]

    def around(k, part, i, step):
        return remote(
            half_of(2 * k + c, part),
            half_of(2 * ((k - step) % 4) + c, part),
            o_send.at[i],
            o_recv.at[i],
            (sp, 2 * lax.rem(y + step + 4, 4) + c),
        )

    def across(k, part):
        shard = half_of(2 * k + c, part)
        return remote(shard, shard, o_send.at[6 + 2 * k + part], o_pair.at[2 * k + part], (sp, partner))

    rounds = [around(0, 1, 0, 1), around(0, 0, 1, -1), around(0, 0, 2, 1), around(0, 1, 3, -1)]
    rounds += [around(3, 1, 4, 1), around(1, 0, 5, -1)]
    landed = ((3, 1), (1, 0), (3, 0), (1, 1), (2, 1), (2, 0))
    acrosses = {(k, part): across(k, part) for k in range(4) for part in (0, 1)}
    for copy in rounds[:4]:
        copy.start()
    acrosses[0, 0].start()
    acrosses[0, 1].start()

    def pass_on(i):
        rounds[i].wait_recv()
        if i < 2:
            rounds[4 + i].start()
        acrosses[landed[i]].start()

    up = jnp.transpose(wkv_up[...].astype(F32))
    for h in range(H):
        wup[h * 64 : (h + 1) * 64] = up[h * 128 : h * 128 + 64].astype(BF)
        wup[192 + h * 64 : 256 + h * 64] = up[h * 128 + 64 : h * 128 + 128].astype(BF)
    lanes = lax.broadcasted_iota(jnp.int32, (16, TB), 1)
    off_c = jnp.sum(jnp.where(lanes == sp, tables[2], 0.0), axis=1, keepdims=True)
    off_s = jnp.sum(jnp.where(lanes == sp, tables[3], 0.0), axis=1, keepdims=True)
    cosine = tables[0] * off_c - tables[1] * off_s
    sine = tables[1] * off_c + tables[0] * off_s
    kcol = column(hk_gain[...].astype(F32), 3)
    qcol = column(hq_gain[...].astype(F32), 3)
    m_ref[...] = jnp.full(m_ref.shape, -1e30, F32)
    acc[...] = jnp.zeros(acc.shape, F32)
    k_ref[...] = jnp.zeros(k_ref.shape, BF)
    v_ref[...] = jnp.zeros(v_ref.shape, BF)
    v_ref[:, :, 64:80, :] = jnp.ones((2, H, 16, v_ref.shape[3]), BF)
    s_ref[...] = jnp.full(s_ref.shape, -3e38, F32)

    gathers += gathered(kvg, 0)
    turned = jnp.transpose(kvg[...].reshape(TB, TB).astype(F32))
    rope = turned[256:288]
    rho = jnp.sum(rope * rope, axis=0, keepdims=True)
    rho_hi = rho.astype(BF).astype(F32)
    rope = rope * kcol[64:96]
    first, second = rope[:16], rope[16:]
    row = lax.broadcasted_iota(jnp.int32, (32, TB), 0)
    last = jnp.where(row == 0, rho_hi, jnp.where(row == 1, rho - rho_hi, 0.0))
    lat[0, 0] = turned[:LH].astype(BF)
    lat[0, 1] = jnp.concatenate(
        [turned[LH:256], first * cosine - second * sine, first * sine + second * cosine, last], axis=0
    ).astype(BF)

    def outgoing(core, s):
        copies = [
            remote(lat.at[s, core], lat.at[t, core], lat_send.at[s, k], lat_recv.at[t], (chip(az, ax), tp))
            for k, (az, ax, t) in enumerate(PLAN[core][s])
        ]
        if s:
            copies.append(
                remote(lat.at[s, core], lat.at[s, core], lat_send.at[s, 5], pair_recv.at[s], (sp, partner))
            )
        return copies

    def serve(point):
        for core in (0, 1):
            slots = SERVICE[core][point]
            if slots:

                @pl.when(c == core)
                def _():
                    for s in slots:
                        if s:
                            remote(
                                lat.at[s, core], lat.at[s, core], lat_send.at[s, 0], lat_recv.at[s], (sp, partner)
                            ).wait_recv()
                        for copy in outgoing(core, s):
                            copy.start()

    for core in (0, 1):

        @pl.when(c == core)
        def _():
            for copy in outgoing(core, 0):
                copy.start()

    gathers += gathered(qg, 2)
    qt = dot(wq_up[...], qg[...].reshape(TB, 512), ((1,), (1,)))
    scale = 96.0 ** -0.5 * LOG2E
    for h in range(H):
        q = qt[h * 96 : (h + 1) * 96]
        q = q * (lax.rsqrt(jnp.mean(q * q, axis=0, keepdims=True) + EPS) * scale) * qcol
        first, second = q[64:80], q[80:96]
        q = jnp.concatenate(
            [
                q[:64] * kcol[:64],
                first * cosine - second * sine,
                first * sine + second * cosine,
                jnp.zeros((32, TB), F32),
            ],
            axis=0,
        )
        qs[h] = jnp.transpose(q).astype(BF)

    for k in range(1, 8):
        exchanged(pool, 4, k)
    halos = [
        remote(
            pool.at[7, pl.ds(32, 16)], halo.at[0], t_sem.at[0, 0], t_sem.at[1, 0], (lax.rem(sp + 1, NB), tp)
        ),
        remote(
            pool.at[0, pl.ds(0, 16)], halo.at[1], t_sem.at[0, 1], t_sem.at[1, 1], (lax.rem(sp + NB - 1, NB), tp)
        ),
    ]
    for copy in halos:
        copy.start()

    def pooling():
        for copy in halos:
            copy.wait_recv()
        mine = pool[...].reshape(TB, 128)
        wide = jnp.concatenate([halo[0], mine, halo[1], jnp.zeros((96, 128), BF)], axis=0)
        half = jnp.left_shift(jnp.int32(1), lax.rem(tp, 4))
        here = lax.broadcasted_iota(jnp.int32, (TB, 512), 0)
        there = lax.broadcasted_iota(jnp.int32, (TB, 512), 1) - 16
        place = there + sp * TB
        band = (there >= here - half) & (there < here + half) & (place >= 0) & (place < LENGTH)
        summed = dot(jnp.where(band, 1.0, 0.0).astype(BF), wide, ((1,), (0,)))
        place = lax.broadcasted_iota(jnp.int32, (TB, 128), 0) + sp * TB
        count = jnp.minimum(place + half, LENGTH) - jnp.maximum(place - half, 0)
        pooled = (summed / count.astype(F32) - mine.astype(F32)).astype(BF)
        mapped = dot(pooled[:, :64], w_mix[0], ((1,), (0,)))
        pool_out[...] = (mapped * p_scale[...].astype(F32)).astype(BF)

    def step(i, carry):
        for k in range(STEPS):

            @pl.when(i == k)
            def _():
                if k == 1:
                    pooling()
                for i_round in W_STEPS.get(k, ()):
                    pass_on(i_round)
                if k:
                    serve(3 * k)
                else:
                    for core in (0, 1):

                        @pl.when(c == core)
                        def _():
                            for s in SERVICE[core][0]:
                                if s:
                                    remote(
                                        lat.at[s, core],
                                        lat.at[s, core],
                                        lat_send.at[s, 0],
                                        lat_recv.at[s],
                                        (sp, partner),
                                    ).wait_recv()
                                    for copy in outgoing(core, s):
                                        copy.start()

                for s in range(PER * k, PER * k + PER):
                    if s:
                        remote(
                            lat.at[s, 1 - c], lat.at[s, 1 - c], lat_send.at[s, 5], pair_recv.at[s], (sp, partner)
                        ).wait_recv()

        def between(h):
            for k in range(STEPS):
                if any(SERVICE[core][3 * k + h] for core in (0, 1)):

                    @pl.when(i == k)
                    def _():
                        serve(3 * k + h)

        v_now, v_last = v_ref.at[lax.rem(i, 2)], v_ref.at[1 - lax.rem(i, 2)]
        for j in range(PER):
            prep(lat[i * PER + j].reshape(2 * LH, TB), wup, k_ref, v_now, j * TB)
        s_0 = dot(qs[0], k_ref[0], ((1,), (0,)))
        soften(2, s_ref[...], m_ref, acc, v_last)
        between(1)
        s_1 = dot(qs[1], k_ref[1], ((1,), (0,)))
        soften(0, s_0, m_ref, acc, v_now)
        between(2)
        s_ref[...] = dot(qs[2], k_ref[2], ((1,), (0,)))
        soften(1, s_1, m_ref, acc, v_now)
        return carry

    lax.fori_loop(0, STEPS, step, 0)

    def head_out(h):
        o = acc[h]
        return (o[:, :64] / o[:, 64:65]).astype(BF)

    cat[0] = jnp.concatenate([head_out(0), head_out(1)], axis=1).reshape(8, OWN, 128)
    tails = exchange(cat.at[0], cat_r.at[0], 6)
    soften(2, s_ref[...], m_ref, acc, v_ref.at[(STEPS - 1) % 2])
    cat[1] = jnp.concatenate([head_out(2), pool_out[...]], axis=1).reshape(8, OWN, 128)
    tails += exchange(cat.at[1], cat_r.at[1], 8)
    lane = lax.broadcasted_iota(jnp.int32, (TB, 128), 1)
    logs = jnp.zeros((TB, 128), F32)
    for h in range(H):
        logs = jnp.where(lane == h, m_ref[h] * LN2 + jnp.log(acc[h][:, 64:65]), logs)
    lse_out[...] = jnp.transpose(logs)[:H]
    sums = dot(cat[0, tp], w_o[c, :128], ((1,), (0,))) + dot(cat[1, tp], w_o[c, 128:], ((1,), (0,)))
    pass_on(4)
    pass_on(5)
    for part in (0, 1):
        for k in (0, 1, 3, 2):
            for core in (1 - c, c):
                if k == 0 and core is c:
                    continue
                member = 2 * lax.rem(y + k, 4) + core
                if core is not c:
                    acrosses[k, part].wait_recv()
                away = lax.rem(member - tp + 8, 8)
                here, kind = cat_r.at[part, member], 6 + 2 * part
                remote(here, here, g_sem.at[kind, away], g_sem.at[kind + 1, away], (sp, partner)).wait_recv()
                rows = slice(128 * part, 128 * part + 128)
                sums = sums + dot(cat_r[part, member], w_o[2 * k + core, rows], ((1,), (0,)))
    out[...] = sums.astype(BF)

    for copy in gathers + halos + tails + rounds + list(acrosses.values()):
        copy.wait_send()
    for core in (0, 1):

        @pl.when(c == core)
        def _():
            for s in range(NB):
                for copy in outgoing(core, s):
                    copy.wait_send()


def write_out(mixed, logs, mixed_out, logs_out):
    mixed_out[...] = mixed[...]
    logs_out[...] = logs[...]


def rotation_tables():
    half = 16
    freqs = 10000.0 ** (-np.arange(half, dtype=np.float64) / half)
    inside = freqs[:, None] * np.arange(TB)[None, :]
    blocks = np.zeros((half, TB))
    blocks[:, :NB] = freqs[:, None] * (TB * np.arange(NB))[None, :]
    return np.stack([np.cos(inside), np.sin(inside), np.cos(blocks), np.sin(blocks)]).astype(np.float32)


def shards(tokens, norm_gain, query_down_weight, query_latent_norm_gain, key_value_down_weight,
           key_value_latent_gain, w_rope_key, w_pool_in, query_up_weight, key_value_up_weight,
           query_gain, key_gain, w_pool_mix, pool_scale, w_out_attn, w_out_pool):
    vmem, anywhere = pl.BlockSpec(memory_space=pltpu.VMEM), pl.BlockSpec(memory_space=pl.ANY)
    dma, n = pltpu.SemaphoreType.DMA, PER * TB
    mixed, logs = pl.pallas_call(
        layer,
        out_shape=(jax.ShapeDtypeStruct((OWN, 2048), BF), jax.ShapeDtypeStruct((H, TB), F32)),
        in_specs=[vmem] + [anywhere] * 4 + [vmem] * 10 + [anywhere] * 2,
        out_specs=(vmem, vmem),
        scratch_shapes=[
            pltpu.VMEM((2048, 512), BF),
            pltpu.VMEM((2048, 256), BF),
            pltpu.VMEM((32, 2048), BF),
            pltpu.VMEM((2048, 512), BF),
            pltpu.VMEM((8, 256, 2048), BF),
            pltpu.VMEM((8, OWN, TB), BF),
            pltpu.VMEM((8, OWN, 512), BF),
            pltpu.VMEM((8, OWN, 128), BF),
            pltpu.VMEM((8, OWN, 128), BF),
            pltpu.VMEM((2, 16, 128), BF),
            pltpu.VMEM((NB, 2, LH, TB), BF),
            pltpu.VMEM((H, TB, 128), BF),
            pltpu.VMEM((H * 128, 256), BF),
            pltpu.VMEM((H, 128, n), BF),
            pltpu.VMEM((2, H, 128, n), BF),
            pltpu.VMEM((H, TB, 128), F32),
            pltpu.VMEM((H, TB, 128), F32),
            pltpu.VMEM((TB, n), F32),
            pltpu.VMEM((TB, 64), BF),
            pltpu.VMEM((2, 8, OWN, 128), BF),
            pltpu.VMEM((2, 8, OWN, 128), BF),
            dma((6,)),
            dma((10, 8)),
            dma((NB, 6)),
            dma((NB,)),
            dma((NB,)),
            dma((14,)),
            dma((6,)),
            dma((8,)),
            dma((2, 2)),
        ],
        compiler_params=pltpu.CompilerParams(
            collective_id=0, has_side_effects=True, vmem_limit_bytes=60 * 2**20
        ),
        name="layer",
    )(
        tokens, query_down_weight, key_value_down_weight, w_rope_key.T, w_pool_in,
        norm_gain.reshape(16, 128), query_latent_norm_gain.reshape(4, 128), key_value_latent_gain.reshape(2, 128),
        query_up_weight.T, key_value_up_weight, query_gain[None], key_gain[None],
        jnp.asarray(rotation_tables()), w_pool_mix, pool_scale[None], w_out_attn, w_out_pool,
    )
    return pl.pallas_call(
        write_out,
        out_shape=(jax.ShapeDtypeStruct((OWN, 2048), BF), jax.ShapeDtypeStruct((H, TB), F32)),
        in_specs=[vmem] * 2,
        out_specs=(vmem, vmem),
        name="write_out",
    )(mixed, logs)


def solution(mesh):
    everywhere = P()
    placed = (
        (P(("sp", "tp"), None),)
        + (everywhere,) * 7
        + (P(None, "tp"),) * 2
        + (everywhere,) * 2
        + (P("tp", None, None), P("tp"), P("tp", None), P("tp", None))
    )
    return jax.shard_map(
        shards,
        mesh=mesh,
        in_specs=placed,
        out_specs=(P(("sp", "tp"), None), P("tp", "sp")),
        check_vma=False,
    )
```

```python
import numpy as np

import jax
import jax.numpy as jnp
from jax import lax
from jax.experimental import pallas as pl
from jax.experimental.pallas import tpu as pltpu
from jax.sharding import PartitionSpec as P

MESH = pl.DeviceIdType.MESH
BF, F32 = jnp.bfloat16, jnp.float32
H = 3
TB = 384
OWN = 48
NB = 32
LH = 160
PER = 4
STEPS = NB // PER
EPS = 1e-6
LOG2E = 1.4426950408889634
LN2 = 0.6931471805599453
LENGTH = NB * TB

ORDER = (
    (0, 0), (1, 0), (-1, 0), (0, 3),
    (0, 1), (2, 0), (1, 3), (-2, 0),
    (-1, 3), (1, 1), (-3, 0), (3, 0),
    (-1, 1), (2, 3), (-1, 2), (0, 2),
    (-2, 3), (1, 2), (4, 0), (3, 3),
    (-2, 1), (-3, 3), (2, 1), (2, 2),
    (-2, 2), (4, 3), (-3, 1), (3, 2),
    (3, 1), (-3, 2), (4, 1), (4, 2),
)
NEAR = ((1, 0), (-1, 0), (0, 1), (0, -1))


def slot_of(dz, dx):
    return ORDER.index(((dz + 3) % 8 - 3, dx % 4))


def forwards(core, dz, dx):
    if core == 0:
        if dz == 0:
            return {0: NEAR, 3: ((0, 1), (1, 0), (-1, 0))}.get(dx, ((1, 0), (-1, 0)))
        if dz in (-1, -2) or (dz == -3 and dx in (0, 1)):
            return ((1, 0),)
        if dz in (1, 2) or (dz == 3 and dx in (2, 3)):
            return ((-1, 0),)
        return ()
    if dx == 0:
        if dz == 0:
            return NEAR
        along = ((1, 0),) if dz in (-1, -2, -3) else ((-1, 0),) if dz in (1, 2) else ()
        return along + ((0, 1), (0, -1))
    if dx == (3 if dz % 2 == 0 else 1):
        return ((0, 1 if dx == 3 else -1),)
    return ()


PLAN = tuple(
    {
        slot_of(dz, dx): tuple((az, ax, slot_of(dz - az, dx - ax)) for az, ax in forwards(core, dz, dx))
        for dz, dx in ORDER
    }
    for core in (0, 1)
)
SERVICE = (
    ((2, 1, 3, 4), (), (), (7, 5, 15, 8, 6), (12, 9), (), (10, 11, 14, 17), (16, 13), (22,), (20,), (23,),
     (18, 19), (24,), (28, 21), (27,), (26,), (25, 29), (), (31,), (30,), (), (), (), ()),
    ((2, 1, 3, 4), (), (), (12, 7, 5, 8, 9, 6), (15, 14), (16, 20), (10, 11, 13, 22), (17,), (24,), (26, 21),
     (18, 28, 19), (), (23,), (29,), (25, 30), (27,), (), (), (31,), (), (), (), (), ()),
)


W_STEPS = {4: (0, 1)}


def dot(a, b, dims):
    return lax.dot_general(a, b, (dims, ((), ())), preferred_element_type=F32)


def remote(src, dst, send, recv, device):
    return pltpu.make_async_remote_copy(
        src_ref=src, dst_ref=dst, send_sem=send, recv_sem=recv, device_id=device, device_id_type=MESH
    )


def norm_rows(v, gain):
    return v * lax.rsqrt(jnp.mean(v * v, axis=-1, keepdims=True) + EPS) * gain


def in_a_row(ref):
    v = ref[...].astype(F32)
    return jnp.concatenate([v[i : i + 1] for i in range(v.shape[0])], axis=1)


def column(row, count):
    n = row.shape[1]
    row = jnp.concatenate([row, jnp.zeros((1, 128 - n), F32)], axis=1)
    return jnp.tile(jnp.transpose(jnp.broadcast_to(row, (128, 128)))[:n], (1, count))


def prep(lat, w_ref, k_ref, v_ref, first):
    n = lat.shape[1]
    cols = slice(first, first + n)
    kv = dot(w_ref[...], lat[:256], ((1,), (0,)))
    rope = lat[256:288].astype(F32)
    rho = lat[288:304].astype(F32)
    rho = rho[0:1] + rho[1:2]
    for h in range(H):
        k = kv[h * 64 : (h + 1) * 64]
        r = lax.rsqrt((jnp.sum(k * k, axis=0, keepdims=True) + rho) * (1.0 / 96) + EPS)
        k_ref[h, 0:64, cols] = (k * r).astype(BF)
        k_ref[h, 64:96, cols] = (rope * r).astype(BF)
        v_ref[h, 0:64, cols] = kv[192 + h * 64 : 256 + h * 64].astype(BF)


def soften(h, s, m_ref, acc, v_ref):
    m_old = m_ref[h]
    m_new = jnp.maximum(m_old, jnp.broadcast_to(jnp.max(s, axis=1, keepdims=True), m_old.shape))
    m_ref[h] = m_new
    p = jnp.exp2(s - jnp.tile(m_new, (1, s.shape[1] // 128))).astype(BF)
    acc[h] = acc[h] * jnp.exp2(m_old - m_new) + dot(p, v_ref[h], ((1,), (1,)))


def layer(
    tok, h_wq, h_wkv, h_wr, h_wp, n_gain, q_gain, kv_gain, wq_up, wkv_up, hq_gain, hk_gain, tables,
    w_mix, p_scale, h_woa, h_wop,
    out, lse_out,
    w_q, w_kv, w_r, w_p, w_o, kvg, qg, psend, pool, halo, lat, qs, wup, k_ref, v_ref, m_ref, acc,
    s_ref, pool_out, cat, cat_r,
    w_sem, g_sem, lat_send, lat_recv, pair_recv, o_send, o_recv, o_pair, t_sem,
):
    sp, tp = lax.axis_index("sp"), lax.axis_index("tp")
    z, x = lax.div(sp, 4), lax.rem(sp, 4)
    y, c = lax.div(tp, 2), lax.rem(tp, 2)
    partner = tp + 1 - 2 * c

    def chip(az, ax):
        return lax.rem(z + az + 8, 8) * 4 + lax.rem(x + ax + 4, 4)

    weights = [
        pltpu.make_async_copy(a, b, w_sem.at[i])
        for i, (a, b) in enumerate(
            (
                (h_wkv, w_kv),
                (h_wr, w_r),
                (h_wq, w_q),
                (h_wp, w_p),
                (h_woa, w_o.at[c, pl.ds(0, 192)]),
                (h_wop, w_o.at[c, pl.ds(192, 64)]),
            )
        )
    ]
    for copy in weights:
        copy.start()

    barrier = pltpu.get_barrier_semaphore()
    friends = [(sp, lax.rem(tp + k, 8)) for k in range(1, 8)]
    friends += [(chip(az, ax), tp) for az, ax in NEAR]
    friends += [(lax.rem(sp + 1, NB), tp), (lax.rem(sp + NB - 1, NB), tp)]
    for friend in friends:
        pl.semaphore_signal(barrier, inc=1, device_id=friend, device_id_type=MESH)

    normed = norm_rows(tok[...].astype(F32), in_a_row(n_gain)).astype(BF)
    weights[0].wait()
    weights[1].wait()
    kv = norm_rows(dot(normed, w_kv[...], ((1,), (0,))), in_a_row(kv_gain))
    rope = dot(normed, w_r[...], ((1,), (1,)))
    kvg[tp] = jnp.concatenate([kv, rope, jnp.zeros((OWN, 96), F32)], axis=1).astype(BF)
    pl.semaphore_wait(barrier, len(friends))

    def spread(rows, kind):
        copies = []
        for k in (2, 1, 3):
            peer = 2 * lax.rem(y + k, 4) + c
            copies.append(remote(rows.at[tp], rows.at[tp], g_sem.at[kind, k], g_sem.at[kind + 1, 4 - k], (sp, peer)))
        copies.append(remote(rows.at[tp], rows.at[tp], g_sem.at[kind, 4], g_sem.at[kind + 1, 4], (sp, partner)))
        for copy in copies:
            copy.start()
        return copies

    def gathered(rows, kind):
        copies = []
        for k in (1, 3, 2):
            peer = 2 * lax.rem(y + k, 4) + c
            remote(rows.at[peer], rows.at[peer], g_sem.at[kind, k], g_sem.at[kind + 1, k], (sp, peer)).wait_recv()
            copies.append(
                remote(rows.at[peer], rows.at[peer], g_sem.at[kind, 4 + k], g_sem.at[kind + 1, 4 + k], (sp, partner))
            )
            copies[-1].start()
        for k in (0, 1, 3, 2):
            peer = 2 * lax.rem(y + k, 4) + 1 - c
            remote(
                rows.at[peer], rows.at[peer], g_sem.at[kind, 4 + k], g_sem.at[kind + 1, 4 + k], (sp, partner)
            ).wait_recv()
        return copies

    gathers = spread(kvg, 0)
    weights[2].wait()
    qg[tp] = norm_rows(dot(normed, w_q[...], ((1,), (0,))), in_a_row(q_gain)).astype(BF)
    gathers += spread(qg, 2)
    weights[3].wait()
    pooled_in = dot(normed, w_p[...], ((1,), (0,))).astype(BF)
    for g in range(8):
        psend[g] = jnp.concatenate([pooled_in[:, g * 64 : (g + 1) * 64], jnp.zeros((OWN, 64), BF)], axis=1)
    pool[tp] = psend[tp]

    def exchange(src, dst, kind):
        copies = []
        for k in (4, 3, 5, 2, 6, 7, 1):
            peer = lax.rem(tp + k, 8)
            copies.append(
                remote(src.at[peer], dst.at[tp], g_sem.at[kind, k], g_sem.at[kind + 1, 8 - k], (sp, peer))
            )
            copies[-1].start()
        return copies

    def exchanged(dst, kind, k):
        peer = lax.rem(tp + k, 8)
        remote(dst.at[peer], dst.at[peer], g_sem.at[kind, k], g_sem.at[kind + 1, k], (sp, peer)).wait_recv()

    gathers += exchange(psend, pool, 4)

    weights[4].wait()
    weights[5].wait()

    def half_of(shard, part):
        return w_o.at[shard, pl.ds(128 * part, 128)]

    def around(k, part, i, step):
        return remote(
            half_of(2 * k + c, part),
            half_of(2 * ((k - step) % 4) + c, part),
            o_send.at[i],
            o_recv.at[i],
            (sp, 2 * lax.rem(y + step + 4, 4) + c),
        )

    def across(k, part):
        shard = half_of(2 * k + c, part)
        return remote(shard, shard, o_send.at[6 + 2 * k + part], o_pair.at[2 * k + part], (sp, partner))

    rounds = [around(0, 1, 0, 1), around(0, 0, 1, -1), around(0, 0, 2, 1), around(0, 1, 3, -1)]
    rounds += [around(3, 1, 4, 1), around(1, 0, 5, -1)]
    landed = ((3, 1), (1, 0), (3, 0), (1, 1), (2, 1), (2, 0))
    acrosses = {(k, part): across(k, part) for k in range(4) for part in (0, 1)}
    for copy in rounds[:4]:
        copy.start()
    acrosses[0, 0].start()
    acrosses[0, 1].start()

    def pass_on(i):
        rounds[i].wait_recv()
        if i < 2:
            rounds[4 + i].start()
        acrosses[landed[i]].start()

    up = jnp.transpose(wkv_up[...].astype(F32))
    for h in range(H):
        wup[h * 64 : (h + 1) * 64] = up[h * 128 : h * 128 + 64].astype(BF)
        wup[192 + h * 64 : 256 + h * 64] = up[h * 128 + 64 : h * 128 + 128].astype(BF)
    lanes = lax.broadcasted_iota(jnp.int32, (16, TB), 1)
    off_c = jnp.sum(jnp.where(lanes == sp, tables[2], 0.0), axis=1, keepdims=True)
    off_s = jnp.sum(jnp.where(lanes == sp, tables[3], 0.0), axis=1, keepdims=True)
    cosine = tables[0] * off_c - tables[1] * off_s
    sine = tables[1] * off_c + tables[0] * off_s
    kcol = column(hk_gain[...].astype(F32), 3)
    qcol = column(hq_gain[...].astype(F32), 3)
    m_ref[...] = jnp.full(m_ref.shape, -1e30, F32)
    acc[...] = jnp.zeros(acc.shape, F32)
    k_ref[...] = jnp.zeros(k_ref.shape, BF)
    v_ref[...] = jnp.zeros(v_ref.shape, BF)
    v_ref[:, :, 64:80, :] = jnp.ones((2, H, 16, v_ref.shape[3]), BF)
    s_ref[...] = jnp.full(s_ref.shape, -3e38, F32)

    gathers += gathered(kvg, 0)
    turned = jnp.transpose(kvg[...].reshape(TB, TB).astype(F32))
    rope = turned[256:288]
    rho = jnp.sum(rope * rope, axis=0, keepdims=True)
    rho_hi = rho.astype(BF).astype(F32)
    rope = rope * kcol[64:96]
    first, second = rope[:16], rope[16:]
    row = lax.broadcasted_iota(jnp.int32, (32, TB), 0)
    last = jnp.where(row == 0, rho_hi, jnp.where(row == 1, rho - rho_hi, 0.0))
    lat[0, 0] = turned[:LH].astype(BF)
    lat[0, 1] = jnp.concatenate(
        [turned[LH:256], first * cosine - second * sine, first * sine + second * cosine, last], axis=0
    ).astype(BF)

    def outgoing(core, s):
        copies = [
            remote(lat.at[s, core], lat.at[t, core], lat_send.at[s, k], lat_recv.at[t], (chip(az, ax), tp))
            for k, (az, ax, t) in enumerate(PLAN[core][s])
        ]
        if s:
            copies.append(
                remote(lat.at[s, core], lat.at[s, core], lat_send.at[s, 5], pair_recv.at[s], (sp, partner))
            )
        return copies

    def serve(point):
        for core in (0, 1):
            slots = SERVICE[core][point]
            if slots:

                @pl.when(c == core)
                def _():
                    for s in slots:
                        if s:
                            remote(
                                lat.at[s, core], lat.at[s, core], lat_send.at[s, 0], lat_recv.at[s], (sp, partner)
                            ).wait_recv()
                        for copy in outgoing(core, s):
                            copy.start()

    for core in (0, 1):

        @pl.when(c == core)
        def _():
            for copy in outgoing(core, 0):
                copy.start()

    gathers += gathered(qg, 2)
    qt = dot(wq_up[...], qg[...].reshape(TB, 512), ((1,), (1,)))
    scale = 96.0 ** -0.5 * LOG2E
    for h in range(H):
        q = qt[h * 96 : (h + 1) * 96]
        q = q * (lax.rsqrt(jnp.mean(q * q, axis=0, keepdims=True) + EPS) * scale) * qcol
        first, second = q[64:80], q[80:96]
        q = jnp.concatenate(
            [
                q[:64] * kcol[:64],
                first * cosine - second * sine,
                first * sine + second * cosine,
                jnp.zeros((32, TB), F32),
            ],
            axis=0,
        )
        qs[h] = jnp.transpose(q).astype(BF)

    for k in range(1, 8):
        exchanged(pool, 4, k)
    halos = [
        remote(
            pool.at[7, pl.ds(32, 16)], halo.at[0], t_sem.at[0, 0], t_sem.at[1, 0], (lax.rem(sp + 1, NB), tp)
        ),
        remote(
            pool.at[0, pl.ds(0, 16)], halo.at[1], t_sem.at[0, 1], t_sem.at[1, 1], (lax.rem(sp + NB - 1, NB), tp)
        ),
    ]
    for copy in halos:
        copy.start()

    def pooling():
        for copy in halos:
            copy.wait_recv()
        mine = pool[...].reshape(TB, 128)
        wide = jnp.concatenate([halo[0], mine, halo[1], jnp.zeros((96, 128), BF)], axis=0)
        half = jnp.left_shift(jnp.int32(1), lax.rem(tp, 4))
        here = lax.broadcasted_iota(jnp.int32, (TB, 512), 0)
        there = lax.broadcasted_iota(jnp.int32, (TB, 512), 1) - 16
        place = there + sp * TB
        band = (there >= here - half) & (there < here + half) & (place >= 0) & (place < LENGTH)
        summed = dot(jnp.where(band, 1.0, 0.0).astype(BF), wide, ((1,), (0,)))
        place = lax.broadcasted_iota(jnp.int32, (TB, 128), 0) + sp * TB
        count = jnp.minimum(place + half, LENGTH) - jnp.maximum(place - half, 0)
        pooled = (summed / count.astype(F32) - mine.astype(F32)).astype(BF)
        mapped = dot(pooled[:, :64], w_mix[0], ((1,), (0,)))
        pool_out[...] = (mapped * p_scale[...].astype(F32)).astype(BF)

    v_own = v_ref.at[1, :, :, pl.ds(0, TB)]
    prep(lat[0].reshape(2 * LH, TB), wup, k_ref, v_own, 0)
    held = [dot(qs[h], k_ref[h, :, :TB], ((1,), (0,))) for h in range(H)]
    for h in range(H):
        soften(h, held[h], m_ref, acc, v_own)

    def arrive(k):
        if k == 1:
            pooling()
        for i_round in W_STEPS.get(k, ()):
            pass_on(i_round)
        serve(3 * k)
        for s in range(PER * k + 1, min(PER * k + PER + 1, NB)):
            remote(
                lat.at[s, 1 - c], lat.at[s, 1 - c], lat_send.at[s, 5], pair_recv.at[s], (sp, partner)
            ).wait_recv()

    def heads(first, count, v_now, v_last, between):
        n = count * TB
        block = jnp.concatenate([lat[first + j].reshape(2 * LH, TB) for j in range(count)], axis=1)
        prep(block, wup, k_ref, v_now, 0)
        s_0 = dot(qs[0], k_ref[0, :, :n], ((1,), (0,)))
        soften(2, s_ref[...], m_ref, acc, v_last)
        between(1)
        s_1 = dot(qs[1], k_ref[1, :, :n], ((1,), (0,)))
        soften(0, s_0, m_ref, acc, v_now)
        between(2)
        s_2 = dot(qs[2], k_ref[2, :, :n], ((1,), (0,)))
        soften(1, s_1, m_ref, acc, v_now)
        return s_2

    def step(i, carry):
        for k in range(STEPS - 1):

            @pl.when(i == k)
            def _():
                arrive(k)

        def between(h):
            for k in range(STEPS - 1):
                if any(SERVICE[core][3 * k + h] for core in (0, 1)):

                    @pl.when(i == k)
                    def _():
                        serve(3 * k + h)

        now = lax.rem(i, 2)
        s_ref[...] = heads(i * PER + 1, PER, v_ref.at[now], v_ref.at[1 - now], between)
        return carry

    lax.fori_loop(0, STEPS - 1, step, 0)
    arrive(STEPS - 1)
    last = (STEPS - 1) * PER + 1
    v_end = v_ref.at[(STEPS - 1) % 2, :, :, pl.ds(0, (NB - last) * TB)]
    s_end = heads(last, NB - last, v_end, v_ref.at[STEPS % 2], lambda h: serve(3 * (STEPS - 1) + h))

    def head_out(h):
        o = acc[h]
        return (o[:, :64] / o[:, 64:65]).astype(BF)

    cat[0] = jnp.concatenate([head_out(0), head_out(1)], axis=1).reshape(8, OWN, 128)
    tails = exchange(cat.at[0], cat_r.at[0], 6)
    pass_on(2)
    pass_on(3)
    soften(2, s_end, m_ref, acc, v_end)
    cat[1] = jnp.concatenate([head_out(2), pool_out[...]], axis=1).reshape(8, OWN, 128)
    tails += exchange(cat.at[1], cat_r.at[1], 8)
    lane = lax.broadcasted_iota(jnp.int32, (TB, 128), 1)
    logs = jnp.zeros((TB, 128), F32)
    for h in range(H):
        logs = jnp.where(lane == h, m_ref[h] * LN2 + jnp.log(acc[h][:, 64:65]), logs)
    lse_out[...] = jnp.transpose(logs)[:H]
    sums = dot(cat[0, tp], w_o[c, :128], ((1,), (0,))) + dot(cat[1, tp], w_o[c, 128:], ((1,), (0,)))
    pass_on(4)
    pass_on(5)
    for part in (0, 1):
        for k in (0, 1, 3, 2):
            for core in (1 - c, c):
                if k == 0 and core is c:
                    continue
                member = 2 * lax.rem(y + k, 4) + core
                if core is not c:
                    acrosses[k, part].wait_recv()
                away = lax.rem(member - tp + 8, 8)
                here, kind = cat_r.at[part, member], 6 + 2 * part
                remote(here, here, g_sem.at[kind, away], g_sem.at[kind + 1, away], (sp, partner)).wait_recv()
                rows = slice(128 * part, 128 * part + 128)
                sums = sums + dot(cat_r[part, member], w_o[2 * k + core, rows], ((1,), (0,)))
    out[...] = sums.astype(BF)

    for copy in gathers + halos + tails + rounds + list(acrosses.values()):
        copy.wait_send()
    for core in (0, 1):

        @pl.when(c == core)
        def _():
            for s in range(NB):
                for copy in outgoing(core, s):
                    copy.wait_send()


def write_out(mixed, logs, mixed_out, logs_out):
    mixed_out[...] = mixed[...]
    logs_out[...] = logs[...]


def rotation_tables():
    half = 16
    freqs = 10000.0 ** (-np.arange(half, dtype=np.float64) / half)
    inside = freqs[:, None] * np.arange(TB)[None, :]
    blocks = np.zeros((half, TB))
    blocks[:, :NB] = freqs[:, None] * (TB * np.arange(NB))[None, :]
    return np.stack([np.cos(inside), np.sin(inside), np.cos(blocks), np.sin(blocks)]).astype(np.float32)


def shards(tokens, norm_gain, query_down_weight, query_latent_norm_gain, key_value_down_weight,
           key_value_latent_gain, w_rope_key, w_pool_in, query_up_weight, key_value_up_weight,
           query_gain, key_gain, w_pool_mix, pool_scale, w_out_attn, w_out_pool):
    vmem, anywhere = pl.BlockSpec(memory_space=pltpu.VMEM), pl.BlockSpec(memory_space=pl.ANY)
    dma, n = pltpu.SemaphoreType.DMA, PER * TB
    mixed, logs = pl.pallas_call(
        layer,
        out_shape=(jax.ShapeDtypeStruct((OWN, 2048), BF), jax.ShapeDtypeStruct((H, TB), F32)),
        in_specs=[vmem] + [anywhere] * 4 + [vmem] * 10 + [anywhere] * 2,
        out_specs=(vmem, vmem),
        scratch_shapes=[
            pltpu.VMEM((2048, 512), BF),
            pltpu.VMEM((2048, 256), BF),
            pltpu.VMEM((32, 2048), BF),
            pltpu.VMEM((2048, 512), BF),
            pltpu.VMEM((8, 256, 2048), BF),
            pltpu.VMEM((8, OWN, TB), BF),
            pltpu.VMEM((8, OWN, 512), BF),
            pltpu.VMEM((8, OWN, 128), BF),
            pltpu.VMEM((8, OWN, 128), BF),
            pltpu.VMEM((2, 16, 128), BF),
            pltpu.VMEM((NB, 2, LH, TB), BF),
            pltpu.VMEM((H, TB, 128), BF),
            pltpu.VMEM((H * 128, 256), BF),
            pltpu.VMEM((H, 128, n), BF),
            pltpu.VMEM((2, H, 128, n), BF),
            pltpu.VMEM((H, TB, 128), F32),
            pltpu.VMEM((H, TB, 128), F32),
            pltpu.VMEM((TB, n), F32),
            pltpu.VMEM((TB, 64), BF),
            pltpu.VMEM((2, 8, OWN, 128), BF),
            pltpu.VMEM((2, 8, OWN, 128), BF),
            dma((6,)),
            dma((10, 8)),
            dma((NB, 6)),
            dma((NB,)),
            dma((NB,)),
            dma((14,)),
            dma((6,)),
            dma((8,)),
            dma((2, 2)),
        ],
        compiler_params=pltpu.CompilerParams(
            collective_id=0, has_side_effects=True, vmem_limit_bytes=60 * 2**20
        ),
        name="layer",
    )(
        tokens, query_down_weight, key_value_down_weight, w_rope_key.T, w_pool_in,
        norm_gain.reshape(16, 128), query_latent_norm_gain.reshape(4, 128), key_value_latent_gain.reshape(2, 128),
        query_up_weight.T, key_value_up_weight, query_gain[None], key_gain[None],
        jnp.asarray(rotation_tables()), w_pool_mix, pool_scale[None], w_out_attn, w_out_pool,
    )
    return pl.pallas_call(
        write_out,
        out_shape=(jax.ShapeDtypeStruct((OWN, 2048), BF), jax.ShapeDtypeStruct((H, TB), F32)),
        in_specs=[vmem] * 2,
        out_specs=(vmem, vmem),
        name="write_out",
    )(mixed, logs)


def solution(mesh):
    everywhere = P()
    placed = (
        (P(("sp", "tp"), None),)
        + (everywhere,) * 7
        + (P(None, "tp"),) * 2
        + (everywhere,) * 2
        + (P("tp", None, None), P("tp"), P("tp", None), P("tp", None))
    )
    return jax.shard_map(
        shards,
        mesh=mesh,
        in_specs=placed,
        out_specs=(P(("sp", "tp"), None), P("tp", "sp")),
        check_vma=False,
    )
```
